128 devices in a mesh: sp: 16 (over z, x), dp: 8 (over y, core).
Axes of the slice: x: 4, y: 4, z: 4, core: 2. Of those that a mesh axis runs over, the one named last changes fastest.
Arguments:
- queries: bfloat16 [8, 2048, 16, 128], P('dp', 'sp'), may hold values from -3.5 to 2
- key_rows: bfloat16 [8, 2048, 16, 128], P('dp', 'sp'), may hold values from -4 to 5.3
- values: bfloat16 [8, 2048, 16, 128], P('dp', 'sp'), may hold values from -6 to 6
- residual: bfloat16 [8, 2048, 4096], P('dp', 'sp'), may hold values from -6 to 6
- out_weight: bfloat16 [2048, 4096], P(None, 'dp'), may hold values from -0.125 to 0.125
- mixer_gain: float32 [4096], replicated, may hold values from 0.1 to 1.9
- expert_gain: float32 [4096], replicated, may hold values from 0.1 to 1.9
- gate_weight: bfloat16 [128, 4096, 512], P(('sp', 'dp')), may hold values from -0.09375 to 0.09375
- up_weight: bfloat16 [128, 4096, 512], P(('sp', 'dp')), may hold values from -0.09375 to 0.09375
- expert_down_matrix: bfloat16 [128, 512, 4096], P(('sp', 'dp')), may hold values from -0.25 to 0.25
- routes: int32 [8, 2048, 2], P('dp', 'sp'), may hold values from 0 to 127, all different within a row; in each aligned block of 128 rows (0 to 127, 128 to 255, ..., all dimensions but the last counted through in order) at most 3 rows name the same one
- route_weight: float32 [8, 2048, 2], P('dp', 'sp'), may hold values from 0.1 to 1
- output_gain: float32 [4096], replicated, may hold values from 0.1 to 1.9
Outputs:
- output: bfloat16 [8, 2048, 4096], P('dp', 'sp')
The draws below stay inside these ranges and needn't reach their ends.
Inputs may be any that keep to these rules, and one draw needn't show every extreme that they name: `routes`: each row names 2 different experts. Among the rows of one device no expert is named more than 3 times, and in every draw some device names some expert exactly 3 times.
All inputs are finite; a program needn't handle non-finite values.
Results may differ from the reference program's by a relative error of at most 0.009.
Values may be sent and summed in bfloat16 or wider, within the bound.
No kernel may reach another device: no remote copies, remote signals or barrier semaphores. Data moves between devices by JAX's collectives and lax.ppermute only.
A program may use at most 192 MiB of HBM per device.

```python
import math
import jax
import jax.numpy as jnp
import numpy as np
from jax import lax

D = 4096
HEADS = 16
HD = 128
FF = 512
TOP = 2
SEG_DEV = 128
BATCH_SEQUENCES = 8
SEQUENCE_LENGTH = 2048
EXPERTS = 128
CAP = 3
N_SP = 16
N_DP = 8


def draw_queries(key, part):
    head_key = jax.random.fold_in(key, 11)
    noise_key = jax.random.fold_in(key, 12)
    spread_key = jax.random.fold_in(key, 13)
    shape = (BATCH_SEQUENCES, SEQUENCE_LENGTH, HEADS, HD)
    slow_level = (math.log(SEQUENCE_LENGTH) + 0.5) / math.sqrt(HD)
    fast_level = (math.log(40.0) + 0.5) / math.sqrt(HD)
    fast_heads = jax.random.uniform(head_key, (HEADS,), jnp.float32) < 0.5
    noise = 0.5 * jax.random.truncated_normal(noise_key, -4.0, 4.0, shape, jnp.float32)
    spread = jax.random.uniform(spread_key, (HEADS,), jnp.float32, 0.9, 1.1)
    tier_value = -jnp.where(fast_heads, fast_level, slow_level) * spread
    return (noise + tier_value[None, None, :, None]).astype(jnp.bfloat16)


def draw_key_rows(key, part):
    noise_key = jax.random.fold_in(key, 21)
    level_key = jax.random.fold_in(key, 22)
    spike_random_key = jax.random.fold_in(key, 23)
    shape = (BATCH_SEQUENCES, SEQUENCE_LENGTH, HEADS, HD)
    blocks = SEQUENCE_LENGTH // SEG_DEV
    noise = jax.random.truncated_normal(noise_key, -4.0, 4.0, shape, jnp.float32)
    tier_value = jnp.exp(jax.random.uniform(level_key, (BATCH_SEQUENCES, blocks), jnp.float32, math.log(0.85), math.log(1.18)))
    tier_value = jnp.repeat(tier_value, SEG_DEV, axis=1)
    sudden_spike = jax.random.uniform(spike_random_key, (BATCH_SEQUENCES, SEQUENCE_LENGTH), jnp.float32) < 6.0 / SEQUENCE_LENGTH
    tier_value = jnp.where(sudden_spike, 0.1, tier_value)
    return (noise + tier_value[:, :, None, None]).astype(jnp.bfloat16)


def shard_levels(stream_key, shape, shards, smallest, largest):
    level, own = 1.0, jax.random.fold_in(stream_key, 6)
    for position, blocks in shards:
        steps = jnp.exp(jax.random.uniform(jax.random.fold_in(own, position), (blocks,), jnp.float32, smallest / len(shards), largest / len(shards)))
        level = level * jnp.repeat(steps, shape[position] // blocks).reshape([-1 if axis == position else 1 for axis in range(len(shape))])
    return level


def shared_out(stream_key, own, number, rows, count, top, limit, lean):
    order = jax.random.permutation(stream_key, count)
    heavy_load, common = load_shares(count, rows * top, limit, lean, True), load_shares(count, rows * top, limit, lean, False)
    places = jnp.arange(count)

    def named(lengths, turn):
        used = int((lengths > 0).sum())
        fixed = max(1, used // 4)
        shifted = fixed + (places - fixed + turn * (used - fixed)) % max(1, count - fixed)
        return jnp.zeros((count,), jnp.int32).at[order[jnp.where(places < fixed, places, shifted)]].set(jnp.asarray(lengths, jnp.int32))

    lengths = jnp.where(number % 4 == 0, named(heavy_load, number // 4), named(common, number - number // 4 - 1))
    mixed = jax.random.permutation(jax.random.fold_in(own, 3), count)
    source_of, taker = mixed[0:count // 2 * 2:2], mixed[1:count // 2 * 2:2]
    margin = jnp.minimum(lengths[source_of] - 1, limit - lengths[taker]) // 2
    margin = jnp.where((source_of == order[0]) | (taker == order[0]) | (lengths[taker] == 0), 0, jnp.maximum(margin, 0))
    shifted = jax.random.randint(jax.random.fold_in(own, 4), (count // 2,), 0, 1 << 20) % (margin + 1)
    lengths = lengths.at[source_of].add(-shifted).at[taker].add(shifted)
    members = jnp.searchsorted(jnp.cumsum(lengths), jnp.arange(rows * top), side="right").astype(jnp.int32)
    grid = members.reshape(top, rows).T
    grid = grid[jax.random.permutation(jax.random.fold_in(own, 1), rows)]
    turn = jax.random.randint(jax.random.fold_in(own, 2), (rows, 1), 0, top)
    return jnp.take_along_axis(grid, (jnp.arange(top)[None, :] + turn) % top, axis=1)


def load_shares(count, total, reach, slope, full):
    weights = [(1 << 20) // math.isqrt(grade ** slope) + 1 for grade in range(1, count + 1)]
    largest = reach if full else min(reach, max(-(-total // count), total * weights[0] // sum(weights)))
    least = 1 if total - largest >= count - 1 else 0
    given, rest = [largest] + [least] * (count - 1), total - largest - least * (count - 1)
    while rest > 0:
        free = [i for i in range(1, count) if given[i] < largest] or [i for i in range(1, count) if given[i] < reach]
        whole, remaining = sum([weights[i] for i in free]), rest
        for i in free:
            addition = min(reach - given[i], max(1, remaining * weights[i] // whole), rest)
            given[i] = given[i] + addition
            rest = rest - addition
    return np.array(given)


def bell_draw(own_key, dims, deviation, bound, shards=(), held_as=jnp.bfloat16):
    loudness = shard_levels(own_key, dims, shards, -0.22, 0.18) if shards else 1.0
    array = jax.random.normal(own_key, dims, jnp.float32) * deviation * loudness
    return jnp.minimum(jnp.maximum(array, -bound), bound).astype(held_as)


def setup_inputs(seed: int = 0) -> dict:
    keys = jax.random.split(jax.random.key(seed), 14)
    queries = draw_queries(jax.random.fold_in(keys[13], 71), 0)
    key_rows = draw_key_rows(jax.random.fold_in(keys[13], 71), 0)
    values = bell_draw(keys[2], (BATCH_SEQUENCES, SEQUENCE_LENGTH, HEADS, HD), 1.0, 6.0, ((0, 8), (1, 16)))
    residual = bell_draw(keys[3], (BATCH_SEQUENCES, SEQUENCE_LENGTH, D), 1.0, 6.0, ((0, 8), (1, 16)))
    out_weight = bell_draw(keys[4], (HEADS * HD, D), (HEADS * HD) ** -0.5, 0.125, ((1, 8),))
    mixer_gain = jnp.clip(1.0 + 0.18 * jax.random.normal(keys[5], (D,), jnp.float32), 0.1, 1.9)
    expert_gain = jnp.clip(1.0 + 0.18 * jax.random.normal(keys[6], (D,), jnp.float32), 0.1, 1.9)
    gate_weight = bell_draw(keys[7], (EXPERTS, D, FF), D ** -0.5, 0.09375, ((0, 128),))
    up_weight = bell_draw(keys[8], (EXPERTS, D, FF), D ** -0.5, 0.09375, ((0, 128),))
    expert_down_matrix = bell_draw(keys[9], (EXPERTS, FF, D), FF ** -0.5, 0.25, ((0, 128),))
    routes_keys = jax.random.split(jax.random.fold_in(keys[10], 1), BATCH_SEQUENCES * SEQUENCE_LENGTH // SEG_DEV)
    routes_turns = jax.random.permutation(jax.random.fold_in(keys[10], 3), BATCH_SEQUENCES * SEQUENCE_LENGTH // SEG_DEV)
    routes = jax.vmap(lambda own, number: shared_out(jax.random.fold_in(keys[10], 2), own, number, SEG_DEV, EXPERTS, TOP, CAP, 2))(routes_keys, routes_turns).reshape((BATCH_SEQUENCES, SEQUENCE_LENGTH, TOP))
    route_weight = jnp.clip(0.1 + 0.9 * jax.random.uniform(keys[11], (BATCH_SEQUENCES, SEQUENCE_LENGTH, TOP), jnp.float32) ** shard_levels(keys[11], (BATCH_SEQUENCES, SEQUENCE_LENGTH, TOP), ((0, 8), (1, 16)), -0.2, 0.2), 0.1, 1.0)
    output_gain = jnp.clip(1.0 + 0.18 * jax.random.normal(keys[12], (D,), jnp.float32), 0.1, 1.9)
    return dict(queries=queries, key_rows=key_rows, values=values, residual=residual, out_weight=out_weight, mixer_gain=mixer_gain, expert_gain=expert_gain, gate_weight=gate_weight, up_weight=up_weight, expert_down_matrix=expert_down_matrix, routes=routes, route_weight=route_weight, output_gain=output_gain)


EPSILON = 1e-06

def normed_token_rows(matrix, gain):
    return matrix * lax.rsqrt(lax.optimization_barrier(jnp.mean(matrix * matrix, axis=-1, keepdims=True)) + EPSILON) * gain

def stick_head(query_rows, key_part, value_part):
    length = query_rows.shape[0]
    block_rows = min(512, length)
    score_scale = HD ** (-0.5)
    pieces = []
    for block_index in range(length // block_rows):
        row_start = block_index * block_rows
        row_stop = row_start + block_rows
        scores = jnp.dot(query_rows[row_start:row_stop], key_part[:row_stop].T, preferred_element_type=jnp.float32) * score_scale
        key_pos = lax.broadcasted_iota(jnp.int32, (block_rows, row_stop), 1)
        query_pos = lax.broadcasted_iota(jnp.int32, (block_rows, row_stop), 0) + row_start
        is_past = key_pos < query_pos
        log_keep = jnp.where(is_past, -jax.nn.softplus(scores), jnp.float32(0.0))
        suffix = lax.cumsum(log_keep, axis=1, reverse=True) - log_keep
        weights = jnp.where(is_past, jnp.exp(jax.nn.log_sigmoid(scores) + suffix), jnp.float32(0.0)).astype(jnp.bfloat16)
        pieces.append(jnp.dot(weights, value_part[:row_stop], preferred_element_type=jnp.float32).astype(jnp.bfloat16))
    return jnp.concatenate(pieces, axis=0)

def reference(queries, key_rows, values, residual, out_weight, mixer_gain, expert_gain, gate_weight, up_weight, expert_down_matrix, routes, route_weight, output_gain):

    def by_head(tensor):
        return jnp.transpose(tensor, (0, 2, 1, 3)).reshape(BATCH_SEQUENCES * HEADS, SEQUENCE_LENGTH, HD)

    def per_pair(operands):
        return stick_head(operands[0], operands[1], operands[2])
    attended = lax.map(per_pair, (by_head(queries), by_head(key_rows), by_head(values)))
    attended = attended.reshape(BATCH_SEQUENCES, HEADS, SEQUENCE_LENGTH, HD).transpose(0, 2, 1, 3).reshape(BATCH_SEQUENCES, SEQUENCE_LENGTH, HEADS * HD)

    def token_side(operands):
        attn_rows, resid_rows = operands
        projected = jnp.dot(attn_rows, out_weight, preferred_element_type=jnp.float32)
        stream = (resid_rows.astype(jnp.float32) + normed_token_rows(projected, mixer_gain)).astype(jnp.bfloat16)
        expert_in = normed_token_rows(stream.astype(jnp.float32), expert_gain).astype(jnp.bfloat16)
        return (stream, expert_in)
    stream, expert_in = lax.map(token_side, (attended, residual))
    tokens = BATCH_SEQUENCES * SEQUENCE_LENGTH
    sources = N_SP * N_DP
    picked_experts = routes.reshape(BATCH_SEQUENCES, N_SP, SEG_DEV * TOP).astype(jnp.int32)
    onehot = (picked_experts[..., None] == jnp.arange(EXPERTS, dtype=jnp.int32)).astype(jnp.int32)
    before = jnp.cumsum(onehot, axis=2) - onehot
    slot_rank = lax.optimization_barrier(jnp.sum(before * onehot, axis=3)).astype(jnp.int32)
    source_id = jnp.arange(N_SP, dtype=jnp.int32)[None, :, None] * N_DP + jnp.arange(BATCH_SEQUENCES, dtype=jnp.int32)[:, None, None]
    token_id = jnp.arange(BATCH_SEQUENCES, dtype=jnp.int32)[:, None, None] * SEQUENCE_LENGTH + jnp.arange(N_SP, dtype=jnp.int32)[None, :, None] * SEG_DEV + jnp.arange(SEG_DEV * TOP, dtype=jnp.int32)[None, None, :] // TOP
    token_id = jnp.broadcast_to(token_id, picked_experts.shape).reshape(-1)
    dest_slot = (source_id * CAP + slot_rank).reshape(-1).astype(jnp.int32)
    expert_flat = picked_experts.reshape(-1)
    expert_slot_tokens = jnp.full((EXPERTS, sources * CAP), tokens, jnp.int32).at[expert_flat, dest_slot].set(token_id)
    padded = jnp.concatenate([expert_in.reshape(tokens, D), jnp.zeros((1, D), jnp.bfloat16)], axis=0)

    def per_expert(operands):
        token_list, gate_part, up_part, down_part = operands
        flat_rows = jnp.take(padded, token_list, axis=0)
        gate_out = jnp.dot(flat_rows, gate_part, preferred_element_type=jnp.float32)
        upward = jnp.dot(flat_rows, up_part, preferred_element_type=jnp.float32)
        hidden = (jax.nn.silu(gate_out) * upward).astype(jnp.bfloat16)
        return jnp.dot(hidden, down_part, preferred_element_type=jnp.float32).astype(jnp.bfloat16)
    served = lax.map(per_expert, (expert_slot_tokens, gate_weight, up_weight, expert_down_matrix))
    gathered = served[expert_flat, dest_slot]
    order = jnp.argsort(token_id * TOP + jnp.arange(tokens * TOP, dtype=jnp.int32) % TOP)
    gathered = gathered[order].reshape(tokens, TOP, D)
    combined = lax.optimization_barrier(jnp.sum(gathered.astype(jnp.float32) * route_weight.reshape(tokens, TOP)[:, :, None], axis=1))
    output = (stream.reshape(tokens, D).astype(jnp.float32) + normed_token_rows(combined, output_gain)).astype(jnp.bfloat16)
    return output.reshape(BATCH_SEQUENCES, SEQUENCE_LENGTH, D)
```

```python
import functools
import math

import jax
import jax.numpy as jnp
from jax import lax
from jax.experimental import pallas as pl
from jax.experimental.pallas import tpu as pltpu
from jax.sharding import Mesh, PartitionSpec as P

EPSILON = 1e-06
F32 = jnp.float32
BF16 = jnp.bfloat16
DP = ("yh", "yl", "c")
ALL = ("sp", "yh", "yl", "c")
VMEM = pl.BlockSpec(memory_space=pltpu.VMEM)
SMEM = pl.BlockSpec(memory_space=pltpu.SMEM)


def attend_kernel(x_ref, o_ref):
    blocks, _, hd = x_ref.shape
    tile = 256
    scale = math.log2(math.e) * hd ** -0.5
    row = lax.broadcasted_iota(jnp.int32, (256, 256), 0) % 128
    col = lax.broadcasted_iota(jnp.int32, (256, 256), 1)
    sums = jnp.where((col >= 128) | (row > col), 1.0, 0.0).astype(BF16)
    query_pos = lax.broadcasted_iota(jnp.int32, (tile, 128), 0)
    key_pos = lax.broadcasted_iota(jnp.int32, (tile, 128), 1)

    def two(block, start):
        return jnp.concatenate(
            [x_ref[2 * block, start : start + 128], x_ref[2 * block + 1, start : start + 128]], axis=0
        )

    for i in range(blocks // 2):
        q = two(i, 0)
        carry, total = None, None
        for j in range(i, -1, -1):
            z = (
                lax.dot_general(q, two(j, 128), (((1,), (1,)), ((), ())), preferred_element_type=F32)
                * scale
            )
            weights = [None, None]
            for half in (1, 0):
                zh = z[:, half * 128 : half * 128 + 128]
                keep = jnp.maximum(zh, 0.0) + jnp.log2(1.0 + jnp.exp2(-jnp.abs(zh)))
                take = zh - keep
                if i == j:
                    past = key_pos + half * 128 < query_pos
                    keep = jnp.where(past, keep, 0.0)
                high = keep.astype(BF16)
                low = (keep - high.astype(F32)).astype(BF16)
                s = jnp.dot(jnp.concatenate([high, low], axis=1), sums, preferred_element_type=F32)
                e = take - s[:, :128]
                if carry is not None:
                    e = e - carry
                w = jnp.exp2(e)
                if i == j:
                    w = jnp.where(past, w, 0.0)
                weights[half] = w.astype(BF16)
                carry = s[:, 128:] if carry is None else carry + s[:, 128:]
            part = jnp.dot(
                jnp.concatenate(weights, axis=1), two(j, 256), preferred_element_type=F32
            )
            total = part if total is None else total + part
        total = total.astype(BF16)
        for copy in range(o_ref.shape[1]):
            o_ref[2 * i, copy] = total[:128]
            o_ref[2 * i + 1, copy] = total[128:]


def attend(x, copies):
    blocks = x.shape[0]
    return pl.pallas_call(
        attend_kernel,
        out_shape=jax.ShapeDtypeStruct((blocks, copies, 128, 128), BF16),
        in_specs=[VMEM],
        out_specs=VMEM,
        compiler_params=pltpu.CompilerParams(vmem_limit_bytes=24 << 20),
        cost_estimate=pl.CostEstimate(
            flops=12 * 10**9, bytes_accessed=3 * 10**6, transcendentals=7 * 10**6
        ),
        name="attend",
    )(x)


def project_kernel(index_ref, x_ref, w0, w1, w2, w3, own_ref, other_ref):
    mine = index_ref[0]
    heads = x_ref.shape[0]
    rows = [
        jnp.concatenate([x_ref[h, member] for h in range(heads)], axis=1)
        for member in (mine, 1 - mine)
    ]
    both = jnp.concatenate(rows, axis=0)
    for k, w_ref in enumerate((w0, w1, w2, w3)):
        for n in range(0, 512, 256):
            out = jnp.dot(both, w_ref[:, n : n + 256], preferred_element_type=F32)
            own_ref[k, :, n : n + 256] = out[:128]
            other_ref[k, :, n : n + 256] = out[128:].astype(BF16)


def project(index, x, ws):
    return pl.pallas_call(
        project_kernel,
        out_shape=(
            jax.ShapeDtypeStruct((4, 128, 512), F32),
            jax.ShapeDtypeStruct((4, 128, 512), BF16),
        ),
        in_specs=[SMEM, VMEM, VMEM, VMEM, VMEM, VMEM],
        out_specs=(VMEM, VMEM),
        compiler_params=pltpu.CompilerParams(vmem_limit_bytes=32 << 20),
        cost_estimate=pl.CostEstimate(flops=2 * 10**9, bytes_accessed=11 * 10**6, transcendentals=0),
        name="project",
    )(index, x, *ws)


def to_rows(inner, outer):
    i = lax.broadcasted_iota(jnp.int32, (256, 256), 0)
    k = lax.broadcasted_iota(jnp.int32, (256, 256), 1)
    return jnp.where(k == (i % inner) * outer + i // inner, 1.0, 0.0).astype(BF16)


def stack_blocks(lower, upper):
    left = jnp.concatenate([lower[:, c * 128 : c * 128 + 128] for c in range(32)], axis=0)
    right = jnp.concatenate([upper[:, c * 128 : c * 128 + 128] for c in range(32)], axis=0)
    return jnp.concatenate([left, right], axis=1)


def mix_kernel(
    place_ref, slot_ref, own_ref, got_ref, residual_ref, mixer_ref, expert_ref,
    stream_ref, out_ref, proj_ref, rows_ref,
):
    for k in range(4):
        proj_ref[:, pl.ds(pl.multiple_of(place_ref[k] * 512, 512), 512)] = own_ref[k]
        proj_ref[:, pl.ds(pl.multiple_of(place_ref[4 + k] * 512, 512), 512)] = got_ref[k].astype(F32)
    spread = to_rows(32, 8)
    width = proj_ref.shape[1]

    @pl.loop(0, proj_ref.shape[0] // 16)
    def _(g):
        at = pl.ds(pl.multiple_of(g * 16, 16), 16)
        p = proj_ref[at, :]
        r = lax.rsqrt(jnp.sum(p * p, axis=1, keepdims=True) * (1.0 / width) + EPSILON)
        stream = (residual_ref[at, :].astype(F32) + p * r * mixer_ref[...]).astype(BF16)
        s = stream.astype(F32)
        r = lax.rsqrt(jnp.sum(s * s, axis=1, keepdims=True) * (1.0 / width) + EPSILON)
        x = s * r * expert_ref[...]
        for value, ref in ((s, stream_ref), (x, rows_ref)):
            spread_out = jnp.dot(
                spread, stack_blocks(value[:8], value[8:]).astype(BF16), preferred_element_type=F32
            ).astype(BF16)
            ref[pl.ds(g * 16, 8)] = spread_out[:, :128].reshape(8, 32, 128)
            ref[pl.ds(g * 16 + 8, 8)] = spread_out[:, 128:].reshape(8, 32, 128)

    experts = out_ref.shape[0]

    @pl.loop(0, experts, unroll=4)
    def _(e):
        for slot in range(out_ref.shape[1] // 32):
            out_ref[e, slot * 32 : slot * 32 + 32, :] = rows_ref[slot_ref[slot * experts + e]]


def mix(place, slots, own, got, residual, mixer_gain, expert_gain):
    tokens, width = residual.shape
    return pl.pallas_call(
        mix_kernel,
        out_shape=(
            jax.ShapeDtypeStruct((tokens, 32, 128), BF16),
            jax.ShapeDtypeStruct((128, slots.shape[0] // 128 * 32, 128), BF16),
        ),
        in_specs=[SMEM, SMEM, VMEM, VMEM, VMEM, VMEM, VMEM],
        out_specs=(VMEM, VMEM),
        scratch_shapes=[pltpu.VMEM((tokens, width), F32), pltpu.VMEM((tokens, 32, 128), BF16)],
        compiler_params=pltpu.CompilerParams(vmem_limit_bytes=24 << 20),
        cost_estimate=pl.CostEstimate(flops=10**9, bytes_accessed=8 * 10**6, transcendentals=0),
        name="mix",
    )(place, slots, own, got, residual, mixer_gain, expert_gain)


def expert_kernel(x_ref, gate_ref, up_ref, down_ref, o_ref, rows_ref, hidden_ref, result_ref):
    sources = x_ref.shape[0]
    slots = x_ref.shape[1] // 32
    gather = to_rows(8, 32)
    spread = to_rows(32, 8)

    for slot in range(slots):

        @pl.loop(0, sources // 16)
        def _(g):
            at = slice(slot * 32, slot * 32 + 32)
            left = x_ref[pl.ds(g * 16, 8), at, :].reshape(256, 128)
            right = x_ref[pl.ds(g * 16 + 8, 8), at, :].reshape(256, 128)
            got = jnp.dot(
                gather, jnp.concatenate([left, right], axis=1), preferred_element_type=F32
            )
            to = pl.ds(pl.multiple_of(slot * sources + g * 16, 16), 16)
            for c in range(32):
                rows_ref[to, c * 128 : c * 128 + 128] = jnp.concatenate(
                    [got[c * 8 : c * 8 + 8, :128], got[c * 8 : c * 8 + 8, 128:]], axis=0
                ).astype(BF16)

    for n in range(0, 512, 256):
        a = jnp.dot(rows_ref[...], gate_ref[:, n : n + 256], preferred_element_type=F32)
        b = jnp.dot(rows_ref[...], up_ref[:, n : n + 256], preferred_element_type=F32)
        hidden_ref[:, n : n + 256] = (a / (1.0 + jnp.exp(-a)) * b).astype(BF16)

    @pl.loop(0, 16)
    def _(n):
        at = pl.ds(pl.multiple_of(n * 256, 256), 256)
        result_ref[:, at] = jnp.dot(hidden_ref[...], down_ref[:, at], preferred_element_type=F32)

    for slot in range(slots):

        @pl.loop(0, sources // 16)
        def _(g):
            base = slot * sources + g * 16
            lower = result_ref[pl.ds(pl.multiple_of(base, 8), 8), :]
            upper = result_ref[pl.ds(pl.multiple_of(base + 8, 8), 8), :]
            out = jnp.dot(
                spread, stack_blocks(lower, upper).astype(BF16), preferred_element_type=F32
            ).astype(BF16)
            at = slice(slot * 32, slot * 32 + 32)
            o_ref[pl.ds(g * 16, 8), at, :] = out[:, :128].reshape(8, 32, 128)
            o_ref[pl.ds(g * 16 + 8, 8), at, :] = out[:, 128:].reshape(8, 32, 128)


def run_experts(x, gate, up, down):
    rows = x.shape[0] * (x.shape[1] // 32)
    return pl.pallas_call(
        expert_kernel,
        out_shape=jax.ShapeDtypeStruct(x.shape, BF16),
        in_specs=[VMEM] * 4,
        out_specs=VMEM,
        scratch_shapes=[
            pltpu.VMEM((rows, 4096), BF16),
            pltpu.VMEM((rows, 512), BF16),
            pltpu.VMEM((rows, 4096), F32),
        ],
        compiler_params=pltpu.CompilerParams(vmem_limit_bytes=48 << 20),
        cost_estimate=pl.CostEstimate(flops=6 * 10**9, bytes_accessed=19 * 10**6, transcendentals=0),
        name="experts",
    )(x, gate, up, down)


def combine_kernel(expert_ref, rank_ref, weight_ref, x_ref, stream_ref, gain_ref, o_ref, out_ref):
    tokens = stream_ref.shape[0]
    gather = to_rows(8, 32)
    gain = gain_ref[...]

    @pl.loop(0, tokens, unroll=8)
    def _(t):
        total = None
        for k in range(2):
            rank = pl.multiple_of(rank_ref[2 * t + k] * 32, 32)
            part = x_ref[expert_ref[2 * t + k], pl.ds(rank, 32), :].astype(F32) * weight_ref[2 * t + k]
            total = part if total is None else total + part
        square = jnp.sum(jnp.sum(total * total, axis=0, keepdims=True), axis=1, keepdims=True)
        r = lax.rsqrt(square * (1.0 / 4096) + EPSILON)
        out_ref[t] = (stream_ref[t].astype(F32) + total * r * gain).astype(BF16)

    @pl.loop(0, tokens // 16)
    def _(g):
        left = out_ref[pl.ds(g * 16, 8)].reshape(256, 128)
        right = out_ref[pl.ds(g * 16 + 8, 8)].reshape(256, 128)
        got = jnp.dot(gather, jnp.concatenate([left, right], axis=1), preferred_element_type=F32)
        to = pl.ds(pl.multiple_of(g * 16, 16), 16)
        for c in range(32):
            o_ref[to, c * 128 : c * 128 + 128] = jnp.concatenate(
                [got[c * 8 : c * 8 + 8, :128], got[c * 8 : c * 8 + 8, 128:]], axis=0
            ).astype(BF16)


def combine(expert, rank, weight, x, stream, gain):
    tokens = stream.shape[0]
    return pl.pallas_call(
        combine_kernel,
        out_shape=jax.ShapeDtypeStruct((tokens, 4096), BF16),
        in_specs=[SMEM, SMEM, SMEM, VMEM, VMEM, VMEM],
        out_specs=VMEM,
        scratch_shapes=[pltpu.VMEM((tokens, 32, 128), BF16)],
        compiler_params=pltpu.CompilerParams(vmem_limit_bytes=24 << 20),
        cost_estimate=pl.CostEstimate(flops=10**9, bytes_accessed=6 * 10**6, transcendentals=0),
        name="combine",
    )(expert, rank, weight, x, stream, gain)


def local(
    queries, key_rows, values, residual, out_weight, mixer_gain, expert_gain,
    gate_weight, up_weight, expert_down_matrix, routes, route_weight, output_gain,
):
    yh, yl, core = (lax.axis_index(a) for a in DP)
    y = yh * 2 + yl

    swap = [(d, d ^ 1) for d in range(8)]
    across = [(d, 6 - d // 2 * 2 + d % 2) for d in range(8)]
    w_near = lax.ppermute(out_weight, DP, across)
    w_core = lax.ppermute(out_weight, DP, swap)
    w_near_core = lax.ppermute(w_near, DP, swap)

    def held(chip):
        return [chip * 2 + core, chip * 2 + 1 - core, 6 - chip * 2 + core, 7 - chip * 2 - core]

    place = jnp.stack(held(y) + held(y ^ 1)).astype(jnp.int32)

    picks = routes[0].reshape(-1)
    count = picks.shape[0]
    onehot = picks[:, None] == lax.broadcasted_iota(jnp.int32, (count, 128), 1)
    earlier = lax.broadcasted_iota(jnp.int32, (count, count), 0) > lax.broadcasted_iota(
        jnp.int32, (count, count), 1
    )
    before = jnp.dot(earlier.astype(BF16), onehot.astype(BF16), preferred_element_type=F32)
    rank = jnp.sum(jnp.where(onehot, before, 0.0), axis=1).astype(jnp.int32)
    token = lax.iota(jnp.int32, count) // routes.shape[2]
    slots = jnp.concatenate(
        [
            jnp.sum(jnp.where(onehot & (rank == s)[:, None], token[:, None], 0), axis=0)
            for s in range(3)
        ]
    ).astype(jnp.int32)

    packed = jnp.concatenate(
        [jnp.transpose(a[0], (1, 0, 2)) for a in (queries, key_rows, values)], axis=1
    )
    by_head = lax.all_to_all(packed, "sp", split_axis=0, concat_axis=0, tiled=True)
    attended = attend(by_head, 2).reshape(32, 128, 128)
    paired = lax.all_to_all(attended, ("sp", "yl"), split_axis=0, concat_axis=0, tiled=True)
    own, other = project(
        yl.reshape(1).astype(jnp.int32), paired.reshape(16, 2, 128, 128),
        (out_weight, w_core, w_near, w_near_core),
    )
    got = lax.ppermute(other, "yl", [(0, 1), (1, 0)])
    stream, outgoing = mix(
        place, slots, own, got, residual[0], mixer_gain.reshape(1, -1), expert_gain.reshape(1, -1)
    )
    arrived = lax.all_to_all(outgoing, ALL, split_axis=0, concat_axis=0, tiled=True)
    result = run_experts(arrived, gate_weight[0], up_weight[0], expert_down_matrix[0])
    returned = lax.all_to_all(result, ALL, split_axis=0, concat_axis=0, tiled=True)
    output = combine(
        picks, rank, route_weight[0].reshape(-1), returned, stream, output_gain.reshape(32, 128)
    )
    return output[None]


def solution(mesh):
    mesh = Mesh(mesh.devices.reshape(16, 2, 2, 2), ALL)
    in_specs = (
        P(DP, "sp", None, None),
        P(DP, "sp", None, None),
        P(DP, "sp", None, None),
        P(DP, "sp", None),
        P(None, DP),
        P(),
        P(),
        P(ALL, None, None),
        P(ALL, None, None),
        P(ALL, None, None),
        P(DP, "sp", None),
        P(DP, "sp", None),
        P(),
    )
    return jax.shard_map(
        local, mesh=mesh, in_specs=in_specs, out_specs=P(DP, "sp", None), check_vma=False
    )
```

```python
import math

import jax
import jax.numpy as jnp
from jax import lax
from jax.experimental import pallas as pl
from jax.experimental.pallas import tpu as pltpu
from jax.sharding import Mesh, PartitionSpec as P


EPSILON = 1e-06
F32 = jnp.float32
BF16 = jnp.bfloat16
DP = ("yh", "yl", "c")
ALL = ("sp", "yh", "yl", "c")
VMEM = pl.BlockSpec(memory_space=pltpu.VMEM)
HBM = pl.BlockSpec(memory_space=pltpu.HBM)
SMEM = pl.BlockSpec(memory_space=pltpu.SMEM)


def attend_kernel(x_ref, o_ref):
    blocks, _, hd = x_ref.shape
    tile = 256
    scale = math.log2(math.e) * hd ** -0.5
    row = lax.broadcasted_iota(jnp.int32, (256, 256), 0) % 128
    col = lax.broadcasted_iota(jnp.int32, (256, 256), 1)
    sums = jnp.where((col >= 128) | (row > col), 1.0, 0.0).astype(BF16)
    query_pos = lax.broadcasted_iota(jnp.int32, (tile, 128), 0)
    key_pos = lax.broadcasted_iota(jnp.int32, (tile, 128), 1)

    def two(block, start):
        return jnp.concatenate(
            [x_ref[2 * block, start : start + 128], x_ref[2 * block + 1, start : start + 128]], axis=0
        )

    for i in range(blocks // 2):
        q = two(i, 0)
        carry, total = None, None
        for j in range(i, -1, -1):
            z = (
                lax.dot_general(q, two(j, 128), (((1,), (1,)), ((), ())), preferred_element_type=F32)
                * scale
            )
            weights = [None, None]
            for half in (1, 0):
                zh = z[:, half * 128 : half * 128 + 128]
                keep = jnp.maximum(zh, 0.0) + jnp.log2(1.0 + jnp.exp2(-jnp.abs(zh)))
                take = zh - keep
                if i == j:
                    past = key_pos + half * 128 < query_pos
                    keep = jnp.where(past, keep, 0.0)
                high = keep.astype(BF16)
                low = (keep - high.astype(F32)).astype(BF16)
                s = jnp.dot(jnp.concatenate([high, low], axis=1), sums, preferred_element_type=F32)
                e = take - s[:, :128]
                if carry is not None:
                    e = e - carry
                w = jnp.exp2(e)
                if i == j:
                    w = jnp.where(past, w, 0.0)
                weights[half] = w.astype(BF16)
                carry = s[:, 128:] if carry is None else carry + s[:, 128:]
            part = jnp.dot(
                jnp.concatenate(weights, axis=1), two(j, 256), preferred_element_type=F32
            )
            total = part if total is None else total + part
        total = total.astype(BF16)
        for copy in range(o_ref.shape[1]):
            o_ref[2 * i, copy] = total[:128]
            o_ref[2 * i + 1, copy] = total[128:]


def attend(x, copies):
    blocks = x.shape[0]
    return pl.pallas_call(
        attend_kernel,
        out_shape=jax.ShapeDtypeStruct((blocks, copies, 128, 128), BF16),
        in_specs=[VMEM],
        out_specs=VMEM,
        compiler_params=pltpu.CompilerParams(vmem_limit_bytes=24 << 20),
        cost_estimate=pl.CostEstimate(
            flops=12 * 10**9, bytes_accessed=3 * 10**6, transcendentals=7 * 10**6
        ),
        name="attend",
    )(x)


def project_kernel(index_ref, x_ref, w0, w1, w2, w3, own_ref, other_ref):
    mine = index_ref[0]
    heads = x_ref.shape[0]
    rows = [
        jnp.concatenate([x_ref[h, member] for h in range(heads)], axis=1)
        for member in (mine, 1 - mine)
    ]
    both = jnp.concatenate(rows, axis=0)
    for k, w_ref in enumerate((w0, w1, w2, w3)):
        for n in range(0, 512, 256):
            out = jnp.dot(both, w_ref[:, n : n + 256], preferred_element_type=F32)
            own_ref[k, :, n : n + 256] = out[:128]
            other_ref[k, :, n : n + 256] = out[128:].astype(BF16)


def project(index, x, ws):
    return pl.pallas_call(
        project_kernel,
        out_shape=(
            jax.ShapeDtypeStruct((4, 128, 512), F32),
            jax.ShapeDtypeStruct((4, 128, 512), BF16),
        ),
        in_specs=[SMEM, VMEM, VMEM, VMEM, VMEM, VMEM],
        out_specs=(VMEM, VMEM),
        compiler_params=pltpu.CompilerParams(vmem_limit_bytes=32 << 20),
        cost_estimate=pl.CostEstimate(flops=2 * 10**9, bytes_accessed=11 * 10**6, transcendentals=0),
        name="project",
    )(index, x, *ws)


def to_rows(inner, outer):
    i = lax.broadcasted_iota(jnp.int32, (256, 256), 0)
    k = lax.broadcasted_iota(jnp.int32, (256, 256), 1)
    return jnp.where(k == (i % inner) * outer + i // inner, 1.0, 0.0).astype(BF16)


def stack_blocks(lower, upper):
    left = jnp.concatenate([lower[:, c * 128 : c * 128 + 128] for c in range(32)], axis=0)
    right = jnp.concatenate([upper[:, c * 128 : c * 128 + 128] for c in range(32)], axis=0)
    return jnp.concatenate([left, right], axis=1)


def mix_kernel(
    place_ref, slot_ref, own_ref, got_ref, residual_ref, mixer_ref, expert_ref,
    stream_ref, out_ref, proj_ref, rows_ref,
):
    for k in range(4):
        proj_ref[:, pl.ds(pl.multiple_of(place_ref[k] * 512, 512), 512)] = own_ref[k]
        proj_ref[:, pl.ds(pl.multiple_of(place_ref[4 + k] * 512, 512), 512)] = got_ref[k].astype(F32)
    spread = to_rows(32, 8)
    width = proj_ref.shape[1]

    @pl.loop(0, proj_ref.shape[0] // 16)
    def _(g):
        at = pl.ds(pl.multiple_of(g * 16, 16), 16)
        p = proj_ref[at, :]
        r = lax.rsqrt(jnp.sum(p * p, axis=1, keepdims=True) * (1.0 / width) + EPSILON)
        stream = (residual_ref[at, :].astype(F32) + p * r * mixer_ref[...]).astype(BF16)
        s = stream.astype(F32)
        r = lax.rsqrt(jnp.sum(s * s, axis=1, keepdims=True) * (1.0 / width) + EPSILON)
        x = s * r * expert_ref[...]
        for value, ref in ((s, stream_ref), (x, rows_ref)):
            spread_out = jnp.dot(
                spread, stack_blocks(value[:8], value[8:]).astype(BF16), preferred_element_type=F32
            ).astype(BF16)
            ref[pl.ds(g * 16, 8)] = spread_out[:, :128].reshape(8, 32, 128)
            ref[pl.ds(g * 16 + 8, 8)] = spread_out[:, 128:].reshape(8, 32, 128)

    experts = out_ref.shape[0]

    @pl.loop(0, experts, unroll=4)
    def _(e):
        for slot in range(out_ref.shape[1] // 32):
            out_ref[e, slot * 32 : slot * 32 + 32, :] = rows_ref[slot_ref[slot * experts + e]]


def mix(place, slots, own, got, residual, mixer_gain, expert_gain):
    tokens, width = residual.shape
    return pl.pallas_call(
        mix_kernel,
        out_shape=(
            jax.ShapeDtypeStruct((tokens, 32, 128), BF16),
            jax.ShapeDtypeStruct((128, slots.shape[0] // 128 * 32, 128), BF16),
        ),
        in_specs=[SMEM, SMEM, VMEM, VMEM, VMEM, VMEM, VMEM],
        out_specs=(VMEM, VMEM),
        scratch_shapes=[pltpu.VMEM((tokens, width), F32), pltpu.VMEM((tokens, 32, 128), BF16)],
        compiler_params=pltpu.CompilerParams(vmem_limit_bytes=24 << 20),
        cost_estimate=pl.CostEstimate(flops=10**9, bytes_accessed=8 * 10**6, transcendentals=0),
        name="mix",
    )(place, slots, own, got, residual, mixer_gain, expert_gain)


def expert_kernel(
    x_hbm, gate_hbm, up_hbm, down_hbm, o_hbm,
    x_ref, gate_ref, up_ref, down_ref, o_ref, rows_ref, hidden_ref, result_ref, in_sem, out_sem,
):
    sources = x_ref.shape[0]
    slots = x_ref.shape[1] // 32
    gather = to_rows(8, 32)
    spread = to_rows(32, 8)
    weights = ((gate_hbm, gate_ref), (up_hbm, up_ref), (down_hbm, down_ref))

    def slot_copy(source, target, sem, slot):
        at = pl.ds(slot * 32, 32)
        return pltpu.make_async_copy(source.at[:, at, :], target.at[:, at, :], sem.at[slot])

    x_copies = [slot_copy(x_hbm, x_ref, in_sem, slot) for slot in range(slots)]
    w_copies = [
        pltpu.make_async_copy(source, target, in_sem.at[slots + k])
        for k, (source, target) in enumerate(weights)
    ]
    for copy in x_copies + w_copies:
        copy.start()

    for slot in range(slots):
        x_copies[slot].wait()

        @pl.loop(0, sources // 16, unroll=8)
        def _(g):
            at = slice(slot * 32, slot * 32 + 32)
            left = x_ref[pl.ds(g * 16, 8), at, :].reshape(256, 128)
            right = x_ref[pl.ds(g * 16 + 8, 8), at, :].reshape(256, 128)
            got = jnp.dot(
                gather, jnp.concatenate([left, right], axis=1), preferred_element_type=F32
            )
            to = pl.ds(pl.multiple_of(slot * sources + g * 16, 16), 16)
            for c in range(32):
                rows_ref[to, c * 128 : c * 128 + 128] = jnp.concatenate(
                    [got[c * 8 : c * 8 + 8, :128], got[c * 8 : c * 8 + 8, 128:]], axis=0
                ).astype(BF16)

    w_copies[0].wait()
    w_copies[1].wait()
    for n in range(0, 512, 256):
        a = jnp.dot(rows_ref[...], gate_ref[:, n : n + 256], preferred_element_type=F32)
        b = jnp.dot(rows_ref[...], up_ref[:, n : n + 256], preferred_element_type=F32)
        hidden_ref[:, n : n + 256] = (a / (1.0 + jnp.exp(-a)) * b).astype(BF16)

    w_copies[2].wait()
    for n in range(0, 4096, 1024):
        result_ref[:, n : n + 1024] = jnp.dot(
            hidden_ref[...], down_ref[:, n : n + 1024], preferred_element_type=F32
        )

    o_copies = [slot_copy(o_ref, o_hbm, out_sem, slot) for slot in range(slots)]
    for slot in range(slots):

        @pl.loop(0, sources // 16, unroll=8)
        def _(g):
            base = slot * sources + g * 16
            lower = result_ref[pl.ds(pl.multiple_of(base, 8), 8), :]
            upper = result_ref[pl.ds(pl.multiple_of(base + 8, 8), 8), :]
            out = jnp.dot(
                spread, stack_blocks(lower, upper).astype(BF16), preferred_element_type=F32
            ).astype(BF16)
            at = slice(slot * 32, slot * 32 + 32)
            o_ref[pl.ds(g * 16, 8), at, :] = out[:, :128].reshape(8, 32, 128)
            o_ref[pl.ds(g * 16 + 8, 8), at, :] = out[:, 128:].reshape(8, 32, 128)

        o_copies[slot].start()
    for copy in o_copies:
        copy.wait()


def run_experts(x, gate, up, down):
    slots = x.shape[1] // 32
    rows = x.shape[0] * slots
    return pl.pallas_call(
        expert_kernel,
        out_shape=pltpu.HBM(x.shape, BF16),
        in_specs=[HBM] * 4,
        out_specs=HBM,
        scratch_shapes=[
            pltpu.VMEM(x.shape, BF16),
            pltpu.VMEM(gate.shape, BF16),
            pltpu.VMEM(up.shape, BF16),
            pltpu.VMEM(down.shape, BF16),
            pltpu.VMEM(x.shape, BF16),
            pltpu.VMEM((rows, 4096), BF16),
            pltpu.VMEM((rows, 512), BF16),
            pltpu.VMEM((rows, 4096), F32),
            pltpu.SemaphoreType.DMA((slots + 3,)),
            pltpu.SemaphoreType.DMA((slots,)),
        ],
        compiler_params=pltpu.CompilerParams(vmem_limit_bytes=48 << 20),
        cost_estimate=pl.CostEstimate(flops=6 * 10**9, bytes_accessed=19 * 10**6, transcendentals=0),
        name="experts",
    )(x, gate, up, down)


def combine_kernel(expert_ref, rank_ref, weight_ref, x_ref, stream_ref, gain_ref, o_ref, out_ref):
    tokens = stream_ref.shape[0]
    gather = to_rows(8, 32)
    gain = gain_ref[...]

    @pl.loop(0, tokens, unroll=8)
    def _(t):
        total = None
        for k in range(2):
            rank = pl.multiple_of(rank_ref[2 * t + k] * 32, 32)
            part = x_ref[expert_ref[2 * t + k], pl.ds(rank, 32), :].astype(F32) * weight_ref[2 * t + k]
            total = part if total is None else total + part
        square = jnp.sum(jnp.sum(total * total, axis=0, keepdims=True), axis=1, keepdims=True)
        r = lax.rsqrt(square * (1.0 / 4096) + EPSILON)
        out_ref[t] = (stream_ref[t].astype(F32) + total * r * gain).astype(BF16)

    @pl.loop(0, tokens // 16)
    def _(g):
        left = out_ref[pl.ds(g * 16, 8)].reshape(256, 128)
        right = out_ref[pl.ds(g * 16 + 8, 8)].reshape(256, 128)
        got = jnp.dot(gather, jnp.concatenate([left, right], axis=1), preferred_element_type=F32)
        to = pl.ds(pl.multiple_of(g * 16, 16), 16)
        for c in range(32):
            o_ref[to, c * 128 : c * 128 + 128] = jnp.concatenate(
                [got[c * 8 : c * 8 + 8, :128], got[c * 8 : c * 8 + 8, 128:]], axis=0
            ).astype(BF16)


def combine(expert, rank, weight, x, stream, gain):
    tokens = stream.shape[0]
    return pl.pallas_call(
        combine_kernel,
        out_shape=jax.ShapeDtypeStruct((tokens, 4096), BF16),
        in_specs=[SMEM, SMEM, SMEM, VMEM, VMEM, VMEM],
        out_specs=VMEM,
        scratch_shapes=[pltpu.VMEM((tokens, 32, 128), BF16)],
        compiler_params=pltpu.CompilerParams(vmem_limit_bytes=24 << 20),
        cost_estimate=pl.CostEstimate(flops=10**9, bytes_accessed=6 * 10**6, transcendentals=0),
        name="combine",
    )(expert, rank, weight, x, stream, gain)


def layer(
    queries, key_rows, values, residual, out_weight, mixer_gain, expert_gain,
    gate_weight, up_weight, expert_down_matrix, routes, route_weight, output_gain,
):
    yh, yl, core = (lax.axis_index(a) for a in DP)
    y = yh * 2 + yl

    swap = [(d, d ^ 1) for d in range(8)]
    across = [(d, 6 - d // 2 * 2 + d % 2) for d in range(8)]
    w_near = lax.ppermute(out_weight, DP, across)
    w_core = lax.ppermute(out_weight, DP, swap)
    w_near_core = lax.ppermute(w_near, DP, swap)

    def held(chip):
        return [chip * 2 + core, chip * 2 + 1 - core, 6 - chip * 2 + core, 7 - chip * 2 - core]

    place = jnp.stack(held(y) + held(y ^ 1)).astype(jnp.int32)

    picks = routes[0].reshape(-1)
    count = picks.shape[0]
    onehot = picks[:, None] == lax.broadcasted_iota(jnp.int32, (count, 128), 1)
    earlier = lax.broadcasted_iota(jnp.int32, (count, count), 0) > lax.broadcasted_iota(
        jnp.int32, (count, count), 1
    )
    before = jnp.dot(earlier.astype(BF16), onehot.astype(BF16), preferred_element_type=F32)
    rank = jnp.sum(jnp.where(onehot, before, 0.0), axis=1).astype(jnp.int32)
    token = lax.iota(jnp.int32, count) // routes.shape[2]
    slots = jnp.concatenate(
        [
            jnp.sum(jnp.where(onehot & (rank == s)[:, None], token[:, None], 0), axis=0)
            for s in range(3)
        ]
    ).astype(jnp.int32)

    packed = jnp.concatenate(
        [jnp.transpose(a[0], (1, 0, 2)) for a in (queries, key_rows, values)], axis=1
    )
    by_head = lax.all_to_all(packed, "sp", split_axis=0, concat_axis=0, tiled=True)
    attended = attend(by_head, 2).reshape(32, 128, 128)
    paired = lax.all_to_all(attended, ("sp", "yl"), split_axis=0, concat_axis=0, tiled=True)
    own, other = project(
        yl.reshape(1).astype(jnp.int32), paired.reshape(16, 2, 128, 128),
        (out_weight, w_core, w_near, w_near_core),
    )
    got = lax.ppermute(other, "yl", [(0, 1), (1, 0)])
    stream, outgoing = mix(
        place, slots, own, got, residual[0], mixer_gain.reshape(1, -1), expert_gain.reshape(1, -1)
    )
    arrived = lax.all_to_all(outgoing, ALL, split_axis=0, concat_axis=0, tiled=True)
    result = run_experts(arrived, gate_weight[0], up_weight[0], expert_down_matrix[0])
    returned = lax.all_to_all(result, ALL, split_axis=0, concat_axis=0, tiled=True)
    output = combine(
        picks, rank, route_weight[0].reshape(-1), returned, stream, output_gain.reshape(32, 128)
    )
    return output[None]


def solution(mesh):
    mesh = Mesh(mesh.devices.reshape(16, 2, 2, 2), ALL)
    in_specs = (
        P(DP, "sp", None, None),
        P(DP, "sp", None, None),
        P(DP, "sp", None, None),
        P(DP, "sp", None),
        P(None, DP),
        P(),
        P(),
        P(ALL, None, None),
        P(ALL, None, None),
        P(ALL, None, None),
        P(DP, "sp", None),
        P(DP, "sp", None),
        P(),
    )
    return jax.shard_map(
        layer, mesh=mesh, in_specs=in_specs, out_specs=P(DP, "sp", None), check_vma=False
    )
```

```python
import functools
import math

import jax
import jax.numpy as jnp
from jax import lax
from jax.experimental import pallas as pl
from jax.experimental.pallas import tpu as pltpu
from jax.sharding import Mesh, PartitionSpec as P


EPSILON = 1e-06
F32 = jnp.float32
BF16 = jnp.bfloat16
DP = ("yh", "yl", "c")
ALL = ("sp", "yh", "yl", "c")
VMEM = pl.BlockSpec(memory_space=pltpu.VMEM)
HBM = pl.BlockSpec(memory_space=pltpu.HBM)
SMEM = pl.BlockSpec(memory_space=pltpu.SMEM)


def attend_kernel(x_ref, o_ref):
    blocks, _, hd = x_ref.shape
    tile = 256
    scale = math.log2(math.e) * hd ** -0.5
    row = lax.broadcasted_iota(jnp.int32, (256, 256), 0) % 128
    col = lax.broadcasted_iota(jnp.int32, (256, 256), 1)
    sums = jnp.where((col >= 128) | (row > col), 1.0, 0.0).astype(BF16)
    query_pos = lax.broadcasted_iota(jnp.int32, (tile, 128), 0)
    key_pos = lax.broadcasted_iota(jnp.int32, (tile, 128), 1)

    def two(block, start):
        return jnp.concatenate(
            [x_ref[2 * block, start : start + 128], x_ref[2 * block + 1, start : start + 128]], axis=0
        )

    for i in range(blocks // 2):
        q = two(i, 0)
        carry, total = None, None
        for j in range(i, -1, -1):
            z = (
                lax.dot_general(q, two(j, 128), (((1,), (1,)), ((), ())), preferred_element_type=F32)
                * scale
            )
            weights = [None, None]
            for half in (1, 0):
                zh = z[:, half * 128 : half * 128 + 128]
                keep = jnp.maximum(zh, 0.0) + jnp.log2(1.0 + jnp.exp2(-jnp.abs(zh)))
                take = zh - keep
                if i == j:
                    past = key_pos + half * 128 < query_pos
                    keep = jnp.where(past, keep, 0.0)
                high = keep.astype(BF16)
                low = (keep - high.astype(F32)).astype(BF16)
                s = jnp.dot(jnp.concatenate([high, low], axis=1), sums, preferred_element_type=F32)
                e = take - s[:, :128]
                if carry is not None:
                    e = e - carry
                w = jnp.exp2(e)
                if i == j:
                    w = jnp.where(past, w, 0.0)
                weights[half] = w.astype(BF16)
                carry = s[:, 128:] if carry is None else carry + s[:, 128:]
            part = jnp.dot(
                jnp.concatenate(weights, axis=1), two(j, 256), preferred_element_type=F32
            )
            total = part if total is None else total + part
        total = total.astype(BF16)
        o_ref[2 * i] = total[:128]
        o_ref[2 * i + 1] = total[128:]


def attend(x):
    blocks = x.shape[0]
    return pl.pallas_call(
        attend_kernel,
        out_shape=jax.ShapeDtypeStruct((blocks, 128, 128), BF16),
        in_specs=[VMEM],
        out_specs=VMEM,
        compiler_params=pltpu.CompilerParams(vmem_limit_bytes=24 << 20),
        cost_estimate=pl.CostEstimate(
            flops=12 * 10**9, bytes_accessed=3 * 10**6, transcendentals=7 * 10**6
        ),
        name="attend",
    )(x)


def project_kernel(own_x_ref, other_x_ref, *refs, parts):
    heads = own_x_ref.shape[0]
    rows = [
        jnp.concatenate([ref[h] for h in range(heads)], axis=1) for ref in (own_x_ref, other_x_ref)
    ]
    both = jnp.concatenate(rows, axis=0)
    own_ref, other_ref = refs[-2:]
    at = 0
    for k, count in enumerate(parts):
        for n in range(0, 512, 256):
            out, start = None, 0
            for ref in refs[at : at + count]:
                stop = start + ref.shape[0]
                part = jnp.dot(
                    both[:, start:stop], ref[:, n : n + 256], preferred_element_type=F32
                )
                out = part if out is None else out + part
                start = stop
            own_ref[k, :, n : n + 256] = out[:128]
            other_ref[k, :, n : n + 256] = out[128:]
        at += count


def project(own_x, other_x, shards):
    parts = tuple(len(shard) for shard in shards)
    weights = [part for shard in shards for part in shard]
    count = len(parts)
    shape = jax.ShapeDtypeStruct((count, 128, 512), F32)
    return pl.pallas_call(
        functools.partial(project_kernel, parts=parts),
        out_shape=(shape, shape),
        in_specs=[VMEM] * (2 + len(weights)),
        out_specs=(VMEM, VMEM),
        compiler_params=pltpu.CompilerParams(vmem_limit_bytes=24 << 20),
        cost_estimate=pl.CostEstimate(
            flops=count * 10**9, bytes_accessed=count * 3 * 10**6, transcendentals=0
        ),
    )(own_x, other_x, *weights)


def to_rows(inner, outer):
    i = lax.broadcasted_iota(jnp.int32, (256, 256), 0)
    k = lax.broadcasted_iota(jnp.int32, (256, 256), 1)
    return jnp.where(k == (i % inner) * outer + i // inner, 1.0, 0.0).astype(BF16)


def stack_blocks(lower, upper):
    left = jnp.concatenate([lower[:, c * 128 : c * 128 + 128] for c in range(32)], axis=0)
    right = jnp.concatenate([upper[:, c * 128 : c * 128 + 128] for c in range(32)], axis=0)
    return jnp.concatenate([left, right], axis=1)


def mix_kernel(
    place_ref, slot_ref, own_ref, own_far_ref, got_ref, got_far_ref, residual_ref, mixer_ref, expert_ref,
    stream_ref, out_ref, proj_ref, rows_ref,
):
    blocks = [ref[k] for ref in (own_ref, own_far_ref, got_ref, got_far_ref) for k in range(ref.shape[0])]
    for k, block in enumerate(blocks):
        proj_ref[:, pl.ds(pl.multiple_of(place_ref[k] * 512, 512), 512)] = block
    spread = to_rows(32, 8)
    width = proj_ref.shape[1]

    @pl.loop(0, proj_ref.shape[0] // 16)
    def _(g):
        at = pl.ds(pl.multiple_of(g * 16, 16), 16)
        p = proj_ref[at, :]
        r = lax.rsqrt(jnp.sum(p * p, axis=1, keepdims=True) * (1.0 / width) + EPSILON)
        stream = (residual_ref[at, :].astype(F32) + p * r * mixer_ref[...]).astype(BF16)
        s = stream.astype(F32)
        r = lax.rsqrt(jnp.sum(s * s, axis=1, keepdims=True) * (1.0 / width) + EPSILON)
        x = s * r * expert_ref[...]
        for value, ref in ((s, stream_ref), (x, rows_ref)):
            spread_out = jnp.dot(
                spread, stack_blocks(value[:8], value[8:]).astype(BF16), preferred_element_type=F32
            ).astype(BF16)
            ref[pl.ds(g * 16, 8)] = spread_out[:, :128].reshape(8, 32, 128)
            ref[pl.ds(g * 16 + 8, 8)] = spread_out[:, 128:].reshape(8, 32, 128)

    experts = out_ref.shape[0]

    @pl.loop(0, experts, unroll=4)
    def _(e):
        for slot in range(out_ref.shape[1] // 32):
            out_ref[e, slot * 32 : slot * 32 + 32, :] = rows_ref[slot_ref[slot * experts + e]]


def mix(place, slots, projected, residual, mixer_gain, expert_gain):
    tokens, width = residual.shape
    return pl.pallas_call(
        mix_kernel,
        out_shape=(
            jax.ShapeDtypeStruct((tokens, 32, 128), BF16),
            jax.ShapeDtypeStruct((128, slots.shape[0] // 128 * 32, 128), BF16),
        ),
        in_specs=[SMEM, SMEM] + [VMEM] * 7,
        out_specs=(VMEM, VMEM),
        scratch_shapes=[pltpu.VMEM((tokens, width), F32), pltpu.VMEM((tokens, 32, 128), BF16)],
        compiler_params=pltpu.CompilerParams(vmem_limit_bytes=24 << 20),
        cost_estimate=pl.CostEstimate(flops=10**9, bytes_accessed=8 * 10**6, transcendentals=0),
        name="mix",
    )(place, slots, *projected, residual, mixer_gain, expert_gain)


def expert_kernel(
    x_hbm, gate_hbm, up_hbm, down_hbm, o_hbm,
    x_ref, gate_ref, up_ref, down_ref, o_ref, rows_ref, hidden_ref, result_ref, in_sem, out_sem,
):
    sources = x_ref.shape[0]
    slots = x_ref.shape[1] // 32
    gather = to_rows(8, 32)
    spread = to_rows(32, 8)
    weights = ((gate_hbm, gate_ref), (up_hbm, up_ref), (down_hbm, down_ref))

    def slot_copy(source, target, sem, slot):
        at = pl.ds(slot * 32, 32)
        return pltpu.make_async_copy(source.at[:, at, :], target.at[:, at, :], sem.at[slot])

    x_copies = [slot_copy(x_hbm, x_ref, in_sem, slot) for slot in range(slots)]
    w_copies = [
        pltpu.make_async_copy(source, target, in_sem.at[slots + k])
        for k, (source, target) in enumerate(weights)
    ]
    for copy in x_copies + w_copies:
        copy.start()

    for slot in range(slots):
        x_copies[slot].wait()

        @pl.loop(0, sources // 16, unroll=8)
        def _(g):
            at = slice(slot * 32, slot * 32 + 32)
            left = x_ref[pl.ds(g * 16, 8), at, :].reshape(256, 128)
            right = x_ref[pl.ds(g * 16 + 8, 8), at, :].reshape(256, 128)
            got = jnp.dot(
                gather, jnp.concatenate([left, right], axis=1), preferred_element_type=F32
            )
            to = pl.ds(pl.multiple_of(slot * sources + g * 16, 16), 16)
            for c in range(32):
                rows_ref[to, c * 128 : c * 128 + 128] = jnp.concatenate(
                    [got[c * 8 : c * 8 + 8, :128], got[c * 8 : c * 8 + 8, 128:]], axis=0
                ).astype(BF16)

    w_copies[0].wait()
    w_copies[1].wait()
    for n in range(0, 512, 256):
        a = jnp.dot(rows_ref[...], gate_ref[:, n : n + 256], preferred_element_type=F32)
        b = jnp.dot(rows_ref[...], up_ref[:, n : n + 256], preferred_element_type=F32)
        hidden_ref[:, n : n + 256] = (a / (1.0 + jnp.exp(-a)) * b).astype(BF16)

    w_copies[2].wait()
    for n in range(0, 4096, 1024):
        result_ref[:, n : n + 1024] = jnp.dot(
            hidden_ref[...], down_ref[:, n : n + 1024], preferred_element_type=F32
        )

    o_copies = [slot_copy(o_ref, o_hbm, out_sem, slot) for slot in range(slots)]
    for slot in range(slots):

        @pl.loop(0, sources // 16, unroll=8)
        def _(g):
            base = slot * sources + g * 16
            lower = result_ref[pl.ds(pl.multiple_of(base, 8), 8), :]
            upper = result_ref[pl.ds(pl.multiple_of(base + 8, 8), 8), :]
            out = jnp.dot(
                spread, stack_blocks(lower, upper).astype(BF16), preferred_element_type=F32
            ).astype(BF16)
            at = slice(slot * 32, slot * 32 + 32)
            o_ref[pl.ds(g * 16, 8), at, :] = out[:, :128].reshape(8, 32, 128)
            o_ref[pl.ds(g * 16 + 8, 8), at, :] = out[:, 128:].reshape(8, 32, 128)

        o_copies[slot].start()
    for copy in o_copies:
        copy.wait()


def run_experts(x, gate, up, down):
    slots = x.shape[1] // 32
    rows = x.shape[0] * slots
    return pl.pallas_call(
        expert_kernel,
        out_shape=pltpu.HBM(x.shape, BF16),
        in_specs=[HBM] * 4,
        out_specs=HBM,
        scratch_shapes=[
            pltpu.VMEM(x.shape, BF16),
            pltpu.VMEM(gate.shape, BF16),
            pltpu.VMEM(up.shape, BF16),
            pltpu.VMEM(down.shape, BF16),
            pltpu.VMEM(x.shape, BF16),
            pltpu.VMEM((rows, 4096), BF16),
            pltpu.VMEM((rows, 512), BF16),
            pltpu.VMEM((rows, 4096), F32),
            pltpu.SemaphoreType.DMA((slots + 3,)),
            pltpu.SemaphoreType.DMA((slots,)),
        ],
        compiler_params=pltpu.CompilerParams(vmem_limit_bytes=48 << 20),
        cost_estimate=pl.CostEstimate(flops=6 * 10**9, bytes_accessed=19 * 10**6, transcendentals=0),
        name="experts",
    )(x, gate, up, down)


def combine_kernel(expert_ref, rank_ref, weight_ref, x_ref, stream_ref, gain_ref, o_ref, out_ref):
    tokens = stream_ref.shape[0]
    gather = to_rows(8, 32)
    gain = gain_ref[...]

    @pl.loop(0, tokens, unroll=8)
    def _(t):
        total = None
        for k in range(2):
            rank = pl.multiple_of(rank_ref[2 * t + k] * 32, 32)
            part = x_ref[expert_ref[2 * t + k], pl.ds(rank, 32), :].astype(F32) * weight_ref[2 * t + k]
            total = part if total is None else total + part
        square = jnp.sum(jnp.sum(total * total, axis=0, keepdims=True), axis=1, keepdims=True)
        r = lax.rsqrt(square * (1.0 / 4096) + EPSILON)
        out_ref[t] = (stream_ref[t].astype(F32) + total * r * gain).astype(BF16)

    @pl.loop(0, tokens // 16)
    def _(g):
        left = out_ref[pl.ds(g * 16, 8)].reshape(256, 128)
        right = out_ref[pl.ds(g * 16 + 8, 8)].reshape(256, 128)
        got = jnp.dot(gather, jnp.concatenate([left, right], axis=1), preferred_element_type=F32)
        to = pl.ds(pl.multiple_of(g * 16, 16), 16)
        for c in range(32):
            o_ref[to, c * 128 : c * 128 + 128] = jnp.concatenate(
                [got[c * 8 : c * 8 + 8, :128], got[c * 8 : c * 8 + 8, 128:]], axis=0
            ).astype(BF16)


def combine(expert, rank, weight, x, stream, gain):
    tokens = stream.shape[0]
    return pl.pallas_call(
        combine_kernel,
        out_shape=jax.ShapeDtypeStruct((tokens, 4096), BF16),
        in_specs=[SMEM, SMEM, SMEM, VMEM, VMEM, VMEM],
        out_specs=VMEM,
        scratch_shapes=[pltpu.VMEM((tokens, 32, 128), BF16)],
        compiler_params=pltpu.CompilerParams(vmem_limit_bytes=24 << 20),
        cost_estimate=pl.CostEstimate(flops=10**9, bytes_accessed=6 * 10**6, transcendentals=0),
        name="combine",
    )(expert, rank, weight, x, stream, gain)


def layer(
    queries, key_rows, values, residual, out_weight, mixer_gain, expert_gain,
    gate_weight, up_weight, expert_down_matrix, routes, route_weight, output_gain,
):
    yh, yl, core = (lax.axis_index(a) for a in DP)
    y = yh * 2 + yl

    right = [(d, (d + 2) % 8) for d in range(8)]
    left = [(d, (d + 6) % 8) for d in range(8)]
    swap = [(0, 1), (1, 0)]
    half = out_weight.shape[0] // 2
    top, bottom = out_weight[:half], out_weight[half:]
    before_top = lax.ppermute(top, DP, right)
    after_bottom = lax.ppermute(bottom, DP, left)
    before_bottom = lax.ppermute(bottom, DP, right)
    after_top = lax.ppermute(top, DP, left)
    far_top = lax.ppermute(before_top, DP, right)
    far_bottom = lax.ppermute(after_bottom, DP, left)

    def held(member):
        return [(y + step) % 4 * 2 + member for step in (0, 3, 1, 2)]

    place = jnp.stack(held(core) + held(1 - core)).astype(jnp.int32)

    picks = routes[0].reshape(-1)
    count = picks.shape[0]
    onehot = picks[:, None] == lax.broadcasted_iota(jnp.int32, (count, 128), 1)
    earlier = lax.broadcasted_iota(jnp.int32, (count, count), 0) > lax.broadcasted_iota(
        jnp.int32, (count, count), 1
    )
    before = jnp.dot(earlier.astype(BF16), onehot.astype(BF16), preferred_element_type=F32)
    rank = jnp.sum(jnp.where(onehot, before, 0.0), axis=1).astype(jnp.int32)
    token = lax.iota(jnp.int32, count) // routes.shape[2]
    slots = jnp.concatenate(
        [
            jnp.sum(jnp.where(onehot & (rank == s)[:, None], token[:, None], 0), axis=0)
            for s in range(3)
        ]
    ).astype(jnp.int32)

    packed = jnp.concatenate(
        [jnp.transpose(a[0], (1, 0, 2)) for a in (queries, key_rows, values)], axis=1
    )
    by_head = lax.all_to_all(packed, "sp", split_axis=0, concat_axis=0, tiled=True)
    attended = attend(by_head)
    own_x = lax.all_to_all(attended, "sp", split_axis=0, concat_axis=0, tiled=True)
    other_x = lax.ppermute(own_x, "c", swap)
    own, other = project(
        own_x, other_x, ((out_weight,), (before_top, before_bottom), (after_top, after_bottom))
    )
    got = lax.ppermute(other, "c", swap)
    own_far, other_far = project(own_x, other_x, ((far_top, far_bottom),))
    got_far = lax.ppermute(other_far, "c", swap)
    stream, outgoing = mix(
        place, slots, (own, own_far, got, got_far), residual[0], mixer_gain.reshape(1, -1),
        expert_gain.reshape(1, -1),
    )
    arrived = lax.all_to_all(outgoing, ALL, split_axis=0, concat_axis=0, tiled=True)
    result = run_experts(arrived, gate_weight[0], up_weight[0], expert_down_matrix[0])
    returned = lax.all_to_all(result, ALL, split_axis=0, concat_axis=0, tiled=True)
    output = combine(
        picks, rank, route_weight[0].reshape(-1), returned, stream, output_gain.reshape(32, 128)
    )
    return output[None]


def solution(mesh):
    mesh = Mesh(mesh.devices.reshape(16, 2, 2, 2), ALL)
    in_specs = (
        P(DP, "sp", None, None),
        P(DP, "sp", None, None),
        P(DP, "sp", None, None),
        P(DP, "sp", None),
        P(None, DP),
        P(),
        P(),
        P(ALL, None, None),
        P(ALL, None, None),
        P(ALL, None, None),
        P(DP, "sp", None),
        P(DP, "sp", None),
        P(),
    )
    return jax.shard_map(
        layer, mesh=mesh, in_specs=in_specs, out_specs=P(DP, "sp", None), check_vma=False
    )
```

```python
import functools
import math

import jax
import jax.numpy as jnp
from jax import lax
from jax.experimental import pallas as pl
from jax.experimental.pallas import tpu as pltpu
from jax.sharding import Mesh, PartitionSpec as P


EPSILON = 1e-06
F32 = jnp.float32
BF16 = jnp.bfloat16
DP = ("yh", "yl", "c")
ALL = ("sp", "yh", "yl", "c")
VMEM = pl.BlockSpec(memory_space=pltpu.VMEM)
ANY = pl.BlockSpec(memory_space=pl.ANY)
HBM = pl.BlockSpec(memory_space=pltpu.HBM)
SMEM = pl.BlockSpec(memory_space=pltpu.SMEM)


def attend_kernel(x_ref, o_ref):
    blocks, _, hd = x_ref.shape
    tile = 256
    scale = math.log2(math.e) * hd ** -0.5
    row = lax.broadcasted_iota(jnp.int32, (256, 256), 0) % 128
    col = lax.broadcasted_iota(jnp.int32, (256, 256), 1)
    sums = jnp.where((col >= 128) | (row > col), 1.0, 0.0).astype(BF16)
    query_pos = lax.broadcasted_iota(jnp.int32, (tile, 128), 0)
    key_pos = lax.broadcasted_iota(jnp.int32, (tile, 128), 1)

    def two(block, start):
        return jnp.concatenate(
            [x_ref[2 * block, start : start + 128], x_ref[2 * block + 1, start : start + 128]], axis=0
        )

    for i in range(blocks // 2):
        q = two(i, 0)
        carry, total = None, None
        for j in range(i, -1, -1):
            z = (
                lax.dot_general(q, two(j, 128), (((1,), (1,)), ((), ())), preferred_element_type=F32)
                * scale
            )
            weights = [None, None]
            for half in (1, 0):
                zh = z[:, half * 128 : half * 128 + 128]
                keep = jnp.maximum(zh, 0.0) + jnp.log2(1.0 + jnp.exp2(-jnp.abs(zh)))
                take = zh - keep
                if i == j:
                    past = key_pos + half * 128 < query_pos
                    keep = jnp.where(past, keep, 0.0)
                high = keep.astype(BF16)
                low = (keep - high.astype(F32)).astype(BF16)
                s = jnp.dot(jnp.concatenate([high, low], axis=1), sums, preferred_element_type=F32)
                e = take - s[:, :128]
                if carry is not None:
                    e = e - carry
                w = jnp.exp2(e)
                if i == j:
                    w = jnp.where(past, w, 0.0)
                weights[half] = w.astype(BF16)
                carry = s[:, 128:] if carry is None else carry + s[:, 128:]
            part = jnp.dot(
                jnp.concatenate(weights, axis=1), two(j, 256), preferred_element_type=F32
            )
            total = part if total is None else total + part
        total = total.astype(BF16)
        o_ref[2 * i] = total[:128]
        o_ref[2 * i + 1] = total[128:]


def attend(x):
    blocks = x.shape[0]
    return pl.pallas_call(
        attend_kernel,
        out_shape=jax.ShapeDtypeStruct((blocks, 128, 128), BF16),
        in_specs=[VMEM],
        out_specs=VMEM,
        compiler_params=pltpu.CompilerParams(vmem_limit_bytes=14 << 20),
        cost_estimate=pl.CostEstimate(
            flops=12 * 10**9, bytes_accessed=3 * 10**6, transcendentals=7 * 10**6
        ),
        name="attend",
    )(x)


def split_kernel(w_hbm, top_ref, bottom_ref, sem):
    half = top_ref.shape[0]
    copies = [
        pltpu.make_async_copy(w_hbm.at[pl.ds(k * half, half), :], ref, sem.at[k])
        for k, ref in enumerate((top_ref, bottom_ref))
    ]
    for copy in copies:
        copy.start()
    for copy in copies:
        copy.wait()


def split(w):
    shape = jax.ShapeDtypeStruct((w.shape[0] // 2, w.shape[1]), w.dtype)
    return pl.pallas_call(
        split_kernel,
        out_shape=(shape, shape),
        in_specs=[HBM],
        out_specs=(VMEM, VMEM),
        scratch_shapes=[pltpu.SemaphoreType.DMA((2,))],
        compiler_params=pltpu.CompilerParams(vmem_limit_bytes=60 << 20),
        cost_estimate=pl.CostEstimate(flops=10**6, bytes_accessed=4 * 10**6, transcendentals=0),
        name="split",
    )(w)


def route_kernel(picks_ref, rank_ref, slot_ref):
    tokens = picks_ref.shape[1]
    experts = 128
    expert = lax.broadcasted_iota(jnp.int32, (experts, tokens), 0)
    one, zero = jnp.ones((), F32), jnp.zeros((), F32)
    earlier = jnp.where(
        lax.broadcasted_iota(jnp.int32, (tokens, tokens), 0)
        < lax.broadcasted_iota(jnp.int32, (tokens, tokens), 1),
        one, zero,
    ).astype(BF16)
    number = lax.broadcasted_iota(jnp.int32, (1, tokens), 1).astype(F32)
    taken, slots = None, None
    for k in range(picks_ref.shape[0]):
        onehot = jnp.where(expert == picks_ref[k : k + 1, :], one, zero)
        before = jnp.dot(onehot.astype(BF16), earlier, preferred_element_type=F32)
        if taken is not None:
            before = before + taken
        rank = jnp.sum(onehot * before, axis=0, keepdims=True)
        count = jnp.sum(onehot, axis=1, keepdims=True)
        taken = count if taken is None else taken + count
        rank_ref[k : k + 1, :] = rank.astype(jnp.int32)
        slot = lax.broadcasted_iota(jnp.int32, (8, tokens), 0).astype(F32)
        held = jnp.where(slot == rank, number, zero).astype(BF16)
        part = lax.dot_general(
            held, onehot.astype(BF16), (((1,), (1,)), ((), ())), preferred_element_type=F32
        )
        slots = part if slots is None else slots + part
    slot_ref[...] = slots.astype(jnp.int32)


def route(picks):
    return pl.pallas_call(
        route_kernel,
        out_shape=(
            jax.ShapeDtypeStruct(picks.shape, jnp.int32),
            jax.ShapeDtypeStruct((8, 128), jnp.int32),
        ),
        in_specs=[VMEM],
        out_specs=(VMEM, VMEM),
        compiler_params=pltpu.CompilerParams(vmem_limit_bytes=4 << 20),
        cost_estimate=pl.CostEstimate(flops=2 * 10**7, bytes_accessed=10**4, transcendentals=0),
        name="route",
    )(picks)


def project_kernel(own_x_ref, other_x_ref, *refs, parts):
    count = sum(parts)
    weights, (own_ref, other_ref, w_ref, sem) = refs[:count], refs[count:]
    copies, at = [], 0
    for k, number in enumerate(parts):
        rows = w_ref.shape[1] // number
        for n in range(number):
            target = w_ref.at[k, pl.ds(n * rows, rows), :]
            copies.append(pltpu.make_async_copy(weights[at], target, sem.at[at]))
            at += 1
    for copy in copies:
        copy.start()
    heads = own_x_ref.shape[0]
    rows = [
        jnp.concatenate([ref[h] for h in range(heads)], axis=1) for ref in (own_x_ref, other_x_ref)
    ]
    both = jnp.concatenate(rows, axis=0)
    at = 0
    for k, number in enumerate(parts):
        for copy in copies[at : at + number]:
            copy.wait()
        at += number
        for n in range(0, 512, 256):
            out = jnp.dot(both, w_ref[k, :, n : n + 256], preferred_element_type=F32)
            own_ref[k, :, n : n + 256] = out[:128]
            other_ref[k, :, n : n + 256] = out[128:]


def project(own_x, other_x, shards):
    parts = tuple(len(shard) for shard in shards)
    weights = [part for shard in shards for part in shard]
    count = len(parts)
    shape = jax.ShapeDtypeStruct((count, 128, 512), F32)
    return pl.pallas_call(
        functools.partial(project_kernel, parts=parts),
        out_shape=(shape, shape),
        in_specs=[VMEM, VMEM] + [ANY] * len(weights),
        out_specs=(VMEM, VMEM),
        scratch_shapes=[
            pltpu.VMEM((count, 2048, 512), BF16),
            pltpu.SemaphoreType.DMA((len(weights),)),
        ],
        compiler_params=pltpu.CompilerParams(vmem_limit_bytes=(5 + 3 * count) << 20),
        cost_estimate=pl.CostEstimate(
            flops=count * 10**9, bytes_accessed=count * 3 * 10**6, transcendentals=0
        ),
    )(own_x, other_x, *weights)


def to_rows(inner, outer):
    i = lax.broadcasted_iota(jnp.int32, (256, 256), 0)
    k = lax.broadcasted_iota(jnp.int32, (256, 256), 1)
    return jnp.where(k == (i % inner) * outer + i // inner, 1.0, 0.0).astype(BF16)


def stack_blocks(lower, upper):
    left = jnp.concatenate([lower[:, c * 128 : c * 128 + 128] for c in range(32)], axis=0)
    right = jnp.concatenate([upper[:, c * 128 : c * 128 + 128] for c in range(32)], axis=0)
    return jnp.concatenate([left, right], axis=1)


def mix_kernel(
    slot_ref, own_ref, own_far_ref, got_ref, got_far_ref, residual_ref, mixer_ref, expert_ref,
    stream_ref, out_ref, proj_ref, rows_ref,
):
    chip, core = lax.axis_index("yh") * 2 + lax.axis_index("yl"), lax.axis_index("c")
    for member, near, far in ((core, own_ref, own_far_ref), (1 - core, got_ref, got_far_ref)):
        for k, step in enumerate((0, 3, 1, 2)):
            at = lax.rem(chip + step, 4) * 1024 + member * 512
            block = near[k] if k < 3 else far[0]
            proj_ref[:, pl.ds(pl.multiple_of(at, 512), 512)] = block
    spread = to_rows(32, 8)
    width = proj_ref.shape[1]

    @pl.loop(0, proj_ref.shape[0] // 16, unroll=8)
    def _(g):
        at = pl.ds(pl.multiple_of(g * 16, 16), 16)
        p = proj_ref[at, :]
        r = lax.rsqrt(jnp.sum(p * p, axis=1, keepdims=True) * (1.0 / width) + EPSILON)
        stream = (residual_ref[at, :].astype(F32) + p * r * mixer_ref[...]).astype(BF16)
        s = stream.astype(F32)
        r = lax.rsqrt(jnp.sum(s * s, axis=1, keepdims=True) * (1.0 / width) + EPSILON)
        x = s * r * expert_ref[...]
        for value, ref in ((s, stream_ref), (x, rows_ref)):
            spread_out = jnp.dot(
                spread, stack_blocks(value[:8], value[8:]).astype(BF16), preferred_element_type=F32
            ).astype(BF16)
            ref[pl.ds(g * 16, 8)] = spread_out[:, :128].reshape(8, 32, 128)
            ref[pl.ds(g * 16 + 8, 8)] = spread_out[:, 128:].reshape(8, 32, 128)

    experts = out_ref.shape[0]

    @pl.loop(0, experts, unroll=16)
    def _(e):
        for slot in range(out_ref.shape[1] // 32):
            out_ref[e, slot * 32 : slot * 32 + 32, :] = rows_ref[slot_ref[slot, e]]


def mix(slots, projected, residual, mixer_gain, expert_gain):
    tokens, width = residual.shape
    return pl.pallas_call(
        mix_kernel,
        out_shape=(
            jax.ShapeDtypeStruct((tokens, 32, 128), BF16),
            jax.ShapeDtypeStruct((128, 96, 128), BF16),
        ),
        in_specs=[SMEM] + [VMEM] * 7,
        out_specs=(VMEM, VMEM),
        scratch_shapes=[pltpu.VMEM((tokens, width), F32), pltpu.VMEM((tokens, 32, 128), BF16)],
        compiler_params=pltpu.CompilerParams(vmem_limit_bytes=14 << 20),
        cost_estimate=pl.CostEstimate(flops=10**9, bytes_accessed=8 * 10**6, transcendentals=0),
        name="mix",
    )(slots, *projected, residual, mixer_gain, expert_gain)


def expert_kernel(
    x_hbm, gate_hbm, up_hbm, down_hbm, o_hbm,
    x_ref, gate_ref, up_ref, down_ref, o_ref, rows_ref, hidden_ref, result_ref, in_sem, out_sem,
):
    sources = x_ref.shape[0]
    slots = x_ref.shape[1] // 32
    gather = to_rows(8, 32)
    spread = to_rows(32, 8)
    weights = ((gate_hbm, gate_ref), (up_hbm, up_ref), (down_hbm, down_ref))

    def slot_copy(source, target, sem, slot):
        at = pl.ds(slot * 32, 32)
        return pltpu.make_async_copy(source.at[:, at, :], target.at[:, at, :], sem.at[slot])

    x_copies = [slot_copy(x_hbm, x_ref, in_sem, slot) for slot in range(slots)]
    w_copies = [
        pltpu.make_async_copy(source, target, in_sem.at[slots + k])
        for k, (source, target) in enumerate(weights)
    ]
    for copy in x_copies + w_copies:
        copy.start()

    for slot in range(slots):
        x_copies[slot].wait()

        @pl.loop(0, sources // 16, unroll=8)
        def _(g):
            at = slice(slot * 32, slot * 32 + 32)
            left = x_ref[pl.ds(g * 16, 8), at, :].reshape(256, 128)
            right = x_ref[pl.ds(g * 16 + 8, 8), at, :].reshape(256, 128)
            got = jnp.dot(
                gather, jnp.concatenate([left, right], axis=1), preferred_element_type=F32
            )
            to = pl.ds(pl.multiple_of(slot * sources + g * 16, 16), 16)
            for c in range(32):
                rows_ref[to, c * 128 : c * 128 + 128] = jnp.concatenate(
                    [got[c * 8 : c * 8 + 8, :128], got[c * 8 : c * 8 + 8, 128:]], axis=0
                ).astype(BF16)

    w_copies[0].wait()
    w_copies[1].wait()
    for n in range(0, 512, 256):
        a = jnp.dot(rows_ref[...], gate_ref[:, n : n + 256], preferred_element_type=F32)
        b = jnp.dot(rows_ref[...], up_ref[:, n : n + 256], preferred_element_type=F32)
        hidden_ref[:, n : n + 256] = (a / (1.0 + jnp.exp(-a)) * b).astype(BF16)

    w_copies[2].wait()
    for n in range(0, 4096, 1024):
        result_ref[:, n : n + 1024] = jnp.dot(
            hidden_ref[...], down_ref[:, n : n + 1024], preferred_element_type=F32
        )

    o_copies = [slot_copy(o_ref, o_hbm, out_sem, slot) for slot in range(slots)]
    for slot in range(slots):

        @pl.loop(0, sources // 16, unroll=8)
        def _(g):
            base = slot * sources + g * 16
            lower = result_ref[pl.ds(pl.multiple_of(base, 8), 8), :]
            upper = result_ref[pl.ds(pl.multiple_of(base + 8, 8), 8), :]
            out = jnp.dot(
                spread, stack_blocks(lower, upper).astype(BF16), preferred_element_type=F32
            ).astype(BF16)
            at = slice(slot * 32, slot * 32 + 32)
            o_ref[pl.ds(g * 16, 8), at, :] = out[:, :128].reshape(8, 32, 128)
            o_ref[pl.ds(g * 16 + 8, 8), at, :] = out[:, 128:].reshape(8, 32, 128)

        o_copies[slot].start()
    for copy in o_copies:
        copy.wait()


def run_experts(x, gate, up, down):
    slots = x.shape[1] // 32
    rows = x.shape[0] * slots
    return pl.pallas_call(
        expert_kernel,
        out_shape=pltpu.HBM(x.shape, BF16),
        in_specs=[HBM] * 4,
        out_specs=HBM,
        scratch_shapes=[
            pltpu.VMEM(x.shape, BF16),
            pltpu.VMEM(gate.shape, BF16),
            pltpu.VMEM(up.shape, BF16),
            pltpu.VMEM(down.shape, BF16),
            pltpu.VMEM(x.shape, BF16),
            pltpu.VMEM((rows, 4096), BF16),
            pltpu.VMEM((rows, 512), BF16),
            pltpu.VMEM((rows, 4096), F32),
            pltpu.SemaphoreType.DMA((slots + 3,)),
            pltpu.SemaphoreType.DMA((slots,)),
        ],
        compiler_params=pltpu.CompilerParams(vmem_limit_bytes=56 << 20),
        cost_estimate=pl.CostEstimate(flops=6 * 10**9, bytes_accessed=19 * 10**6, transcendentals=0),
        name="experts",
    )(x, gate, up, down)


def combine_kernel(expert_ref, rank_ref, weight_ref, x_ref, stream_ref, gain_ref, o_ref, out_ref):
    tokens = stream_ref.shape[0]
    gather = to_rows(8, 32)
    gain = gain_ref[...]

    @pl.loop(0, tokens, unroll=16)
    def _(t):
        total = None
        for k in range(2):
            rank = pl.multiple_of(rank_ref[k, t] * 32, 32)
            part = x_ref[expert_ref[k, t], pl.ds(rank, 32), :].astype(F32) * weight_ref[k, t]
            total = part if total is None else total + part
        square = jnp.sum(jnp.sum(total * total, axis=0, keepdims=True), axis=1, keepdims=True)
        r = lax.rsqrt(square * (1.0 / 4096) + EPSILON)
        out_ref[t] = (stream_ref[t].astype(F32) + total * r * gain).astype(BF16)

    @pl.loop(0, tokens // 16, unroll=8)
    def _(g):
        left = out_ref[pl.ds(g * 16, 8)].reshape(256, 128)
        right = out_ref[pl.ds(g * 16 + 8, 8)].reshape(256, 128)
        got = jnp.dot(gather, jnp.concatenate([left, right], axis=1), preferred_element_type=F32)
        to = pl.ds(pl.multiple_of(g * 16, 16), 16)
        for c in range(32):
            o_ref[to, c * 128 : c * 128 + 128] = jnp.concatenate(
                [got[c * 8 : c * 8 + 8, :128], got[c * 8 : c * 8 + 8, 128:]], axis=0
            ).astype(BF16)


def combine(expert, rank, weight, x, stream, gain):
    tokens = stream.shape[0]
    return pl.pallas_call(
        combine_kernel,
        out_shape=jax.ShapeDtypeStruct((tokens, 4096), BF16),
        in_specs=[SMEM, SMEM, SMEM, VMEM, VMEM, VMEM],
        out_specs=VMEM,
        scratch_shapes=[pltpu.VMEM((tokens, 32, 128), BF16)],
        compiler_params=pltpu.CompilerParams(vmem_limit_bytes=14 << 20),
        cost_estimate=pl.CostEstimate(flops=10**9, bytes_accessed=6 * 10**6, transcendentals=0),
        name="combine",
    )(expert, rank, weight, x, stream, gain)


def layer(
    queries, key_rows, values, residual, out_weight, mixer_gain, expert_gain,
    gate_weight, up_weight, expert_down_matrix, routes, route_weight, output_gain,
):
    right = [(d, (d + 2) % 8) for d in range(8)]
    left = [(d, (d + 6) % 8) for d in range(8)]
    swap = [(0, 1), (1, 0)]
    top, bottom = split(out_weight)
    before_top = lax.ppermute(top, DP, right)
    after_bottom = lax.ppermute(bottom, DP, left)
    before_bottom = lax.ppermute(bottom, DP, right)
    after_top = lax.ppermute(top, DP, left)
    far_top = lax.ppermute(before_top, DP, right)
    far_bottom = lax.ppermute(after_bottom, DP, left)

    picks = jnp.transpose(routes[0])
    rank, slots = route(picks)

    packed = jnp.concatenate(
        [jnp.transpose(a[0], (1, 0, 2)) for a in (queries, key_rows, values)], axis=1
    )
    by_head = lax.all_to_all(packed, "sp", split_axis=0, concat_axis=0, tiled=True)
    attended = attend(by_head)
    own_x = lax.all_to_all(attended, "sp", split_axis=0, concat_axis=0, tiled=True)
    other_x = lax.ppermute(own_x, "c", swap)
    own, other = project(
        own_x, other_x, ((top, bottom), (before_top, before_bottom), (after_top, after_bottom))
    )
    got = lax.ppermute(other, "c", swap)
    own_far, other_far = project(own_x, other_x, ((far_top, far_bottom),))
    got_far = lax.ppermute(other_far, "c", swap)
    stream, outgoing = mix(
        slots, (own, own_far, got, got_far), residual[0], mixer_gain.reshape(1, -1),
        expert_gain.reshape(1, -1),
    )
    arrived = lax.all_to_all(outgoing, ALL, split_axis=0, concat_axis=0, tiled=True)
    result = run_experts(arrived, gate_weight[0], up_weight[0], expert_down_matrix[0])
    returned = lax.all_to_all(result, ALL, split_axis=0, concat_axis=0, tiled=True)
    output = combine(
        picks, rank, jnp.transpose(route_weight[0]), returned, stream, output_gain.reshape(32, 128)
    )
    return output[None]


def solution(mesh):
    mesh = Mesh(mesh.devices.reshape(16, 2, 2, 2), ALL)
    in_specs = (
        P(DP, "sp", None, None),
        P(DP, "sp", None, None),
        P(DP, "sp", None, None),
        P(DP, "sp", None),
        P(None, DP),
        P(),
        P(),
        P(ALL, None, None),
        P(ALL, None, None),
        P(ALL, None, None),
        P(DP, "sp", None),
        P(DP, "sp", None),
        P(),
    )
    return jax.shard_map(
        layer, mesh=mesh, in_specs=in_specs, out_specs=P(DP, "sp", None), check_vma=False
    )
```

```python
import math

import jax
import jax.numpy as jnp
from jax import lax
from jax.experimental import pallas as pl
from jax.experimental.pallas import tpu as pltpu
from jax.sharding import Mesh, PartitionSpec as P


EPSILON = 1e-06
F32 = jnp.float32
BF16 = jnp.bfloat16
DP = ("yh", "yl", "c")
ALL = ("sp", "yh", "yl", "c")
VMEM = pl.BlockSpec(memory_space=pltpu.VMEM)
ANY = pl.BlockSpec(memory_space=pl.ANY)
HBM = pl.BlockSpec(memory_space=pltpu.HBM)
SMEM = pl.BlockSpec(memory_space=pltpu.SMEM)


def attend_kernel(x_ref, o_ref):
    blocks, _, hd = x_ref.shape
    tile = 256
    scale = math.log2(math.e) * hd ** -0.5
    row = lax.broadcasted_iota(jnp.int32, (256, 256), 0) % 128
    col = lax.broadcasted_iota(jnp.int32, (256, 256), 1)
    sums = jnp.where((col >= 128) | (row > col), 1.0, 0.0).astype(BF16)
    query_pos = lax.broadcasted_iota(jnp.int32, (tile, 128), 0)
    key_pos = lax.broadcasted_iota(jnp.int32, (tile, 128), 1)

    def two(block, start):
        return jnp.concatenate(
            [x_ref[2 * block, start : start + 128], x_ref[2 * block + 1, start : start + 128]], axis=0
        )

    for i in range(blocks // 2):
        q = two(i, 0)
        carry, total = None, None
        for j in range(i, -1, -1):
            z = (
                lax.dot_general(q, two(j, 128), (((1,), (1,)), ((), ())), preferred_element_type=F32)
                * scale
            )
            weights = [None, None]
            for half in (1, 0):
                zh = z[:, half * 128 : half * 128 + 128]
                keep = jnp.maximum(zh, 0.0) + jnp.log2(1.0 + jnp.exp2(-jnp.abs(zh)))
                take = zh - keep
                if i == j:
                    past = key_pos + half * 128 < query_pos
                    keep = jnp.where(past, keep, 0.0)
                high = keep.astype(BF16)
                low = (keep - high.astype(F32)).astype(BF16)
                s = jnp.dot(jnp.concatenate([high, low], axis=1), sums, preferred_element_type=F32)
                e = take - s[:, :128]
                if carry is not None:
                    e = e - carry
                w = jnp.exp2(e)
                if i == j:
                    w = jnp.where(past, w, 0.0)
                weights[half] = w.astype(BF16)
                carry = s[:, 128:] if carry is None else carry + s[:, 128:]
            part = jnp.dot(
                jnp.concatenate(weights, axis=1), two(j, 256), preferred_element_type=F32
            )
            total = part if total is None else total + part
        total = total.astype(BF16)
        o_ref[2 * i] = total[:128]
        o_ref[2 * i + 1] = total[128:]


def attend(x):
    blocks = x.shape[0]
    return pl.pallas_call(
        attend_kernel,
        out_shape=jax.ShapeDtypeStruct((blocks, 128, 128), BF16),
        in_specs=[VMEM],
        out_specs=VMEM,
        compiler_params=pltpu.CompilerParams(vmem_limit_bytes=14 << 20),
        cost_estimate=pl.CostEstimate(
            flops=12 * 10**9, bytes_accessed=3 * 10**6, transcendentals=7 * 10**6
        ),
        name="attend",
    )(x)


def route_kernel(picks_ref, rank_ref, slot_ref):
    tokens = picks_ref.shape[1]
    experts = 128
    expert = lax.broadcasted_iota(jnp.int32, (experts, tokens), 0)
    one, zero = jnp.ones((), F32), jnp.zeros((), F32)
    earlier = jnp.where(
        lax.broadcasted_iota(jnp.int32, (tokens, tokens), 0)
        < lax.broadcasted_iota(jnp.int32, (tokens, tokens), 1),
        one, zero,
    ).astype(BF16)
    number = lax.broadcasted_iota(jnp.int32, (1, tokens), 1).astype(F32)
    taken, slots = None, None
    for k in range(picks_ref.shape[0]):
        onehot = jnp.where(expert == picks_ref[k : k + 1, :], one, zero)
        before = jnp.dot(onehot.astype(BF16), earlier, preferred_element_type=F32)
        if taken is not None:
            before = before + taken
        rank = jnp.sum(onehot * before, axis=0, keepdims=True)
        count = jnp.sum(onehot, axis=1, keepdims=True)
        taken = count if taken is None else taken + count
        rank_ref[k : k + 1, :] = rank.astype(jnp.int32)
        slot = lax.broadcasted_iota(jnp.int32, (8, tokens), 0).astype(F32)
        held = jnp.where(slot == rank, number, zero).astype(BF16)
        part = lax.dot_general(
            held, onehot.astype(BF16), (((1,), (1,)), ((), ())), preferred_element_type=F32
        )
        slots = part if slots is None else slots + part
    slot_ref[...] = slots.astype(jnp.int32)


def route(picks):
    return pl.pallas_call(
        route_kernel,
        out_shape=(
            jax.ShapeDtypeStruct(picks.shape, jnp.int32),
            jax.ShapeDtypeStruct((8, 128), jnp.int32),
        ),
        in_specs=[VMEM],
        out_specs=(VMEM, VMEM),
        compiler_params=pltpu.CompilerParams(vmem_limit_bytes=4 << 20),
        cost_estimate=pl.CostEstimate(flops=2 * 10**7, bytes_accessed=10**4, transcendentals=0),
        name="route",
    )(picks)


def project_kernel(own_x_ref, other_x_ref, *refs):
    *weights, own_ref, other_ref, w_ref, sem = refs
    copies = [
        pltpu.make_async_copy(ref, w_ref.at[k], sem.at[k]) for k, ref in enumerate(weights)
    ]
    for copy in copies:
        copy.start()
    heads = own_x_ref.shape[0]
    rows = [
        jnp.concatenate([ref[h] for h in range(heads)], axis=1) for ref in (own_x_ref, other_x_ref)
    ]
    both = jnp.concatenate(rows, axis=0)
    for k, copy in enumerate(copies):
        copy.wait()
        for n in range(0, 512, 256):
            out = jnp.dot(both, w_ref[k, :, n : n + 256], preferred_element_type=F32)
            own_ref[k, :, n : n + 256] = out[:128]
            other_ref[k, :, n : n + 256] = out[128:]


def project(own_x, other_x, weights):
    count = len(weights)
    shape = jax.ShapeDtypeStruct((count, 128, 512), F32)
    return pl.pallas_call(
        project_kernel,
        out_shape=(shape, shape),
        in_specs=[VMEM, VMEM] + [ANY] * count,
        out_specs=(VMEM, VMEM),
        scratch_shapes=[
            pltpu.VMEM((count, 2048, 512), BF16),
            pltpu.SemaphoreType.DMA((count,)),
        ],
        compiler_params=pltpu.CompilerParams(vmem_limit_bytes=(5 + 3 * count) << 20),
        cost_estimate=pl.CostEstimate(
            flops=count * 10**9, bytes_accessed=count * 3 * 10**6, transcendentals=0
        ),
    )(own_x, other_x, *weights)


def to_rows(inner, outer):
    i = lax.broadcasted_iota(jnp.int32, (256, 256), 0)
    k = lax.broadcasted_iota(jnp.int32, (256, 256), 1)
    return jnp.where(k == (i % inner) * outer + i // inner, 1.0, 0.0).astype(BF16)


def stack_blocks(lower, upper):
    left = jnp.concatenate([lower[:, c * 128 : c * 128 + 128] for c in range(32)], axis=0)
    right = jnp.concatenate([upper[:, c * 128 : c * 128 + 128] for c in range(32)], axis=0)
    return jnp.concatenate([left, right], axis=1)


def mix_kernel(
    slot_ref, own_ref, own_far_ref, got_ref, got_far_ref, residual_ref, mixer_ref, expert_ref,
    stream_ref, out_ref, proj_ref, rows_ref,
):
    chip, core = lax.axis_index("yh") * 2 + lax.axis_index("yl"), lax.axis_index("c")
    for member, near, far in ((core, own_ref, own_far_ref), (1 - core, got_ref, got_far_ref)):
        for k, step in enumerate((0, 3 - 2 * member, 1 + 2 * member, 2)):
            at = lax.rem(chip + step, 4) * 1024 + member * 512
            block = near[k] if k < 3 else far[0]
            proj_ref[:, pl.ds(pl.multiple_of(at, 512), 512)] = block
    spread = to_rows(32, 8)
    width = proj_ref.shape[1]

    @pl.loop(0, proj_ref.shape[0] // 16, unroll=8)
    def _(g):
        at = pl.ds(pl.multiple_of(g * 16, 16), 16)
        p = proj_ref[at, :]
        r = lax.rsqrt(jnp.sum(p * p, axis=1, keepdims=True) * (1.0 / width) + EPSILON)
        stream = (residual_ref[at, :].astype(F32) + p * r * mixer_ref[...]).astype(BF16)
        s = stream.astype(F32)
        r = lax.rsqrt(jnp.sum(s * s, axis=1, keepdims=True) * (1.0 / width) + EPSILON)
        x = s * r * expert_ref[...]
        for value, ref in ((s, stream_ref), (x, rows_ref)):
            spread_out = jnp.dot(
                spread, stack_blocks(value[:8], value[8:]).astype(BF16), preferred_element_type=F32
            ).astype(BF16)
            ref[pl.ds(g * 16, 8)] = spread_out[:, :128].reshape(8, 32, 128)
            ref[pl.ds(g * 16 + 8, 8)] = spread_out[:, 128:].reshape(8, 32, 128)

    experts = out_ref.shape[0]

    @pl.loop(0, experts, unroll=16)
    def _(e):
        for slot in range(out_ref.shape[1] // 32):
            out_ref[e, slot * 32 : slot * 32 + 32, :] = rows_ref[slot_ref[slot, e]]


def mix(slots, projected, residual, mixer_gain, expert_gain):
    tokens, width = residual.shape
    return pl.pallas_call(
        mix_kernel,
        out_shape=(
            jax.ShapeDtypeStruct((tokens, 32, 128), BF16),
            jax.ShapeDtypeStruct((128, 96, 128), BF16),
        ),
        in_specs=[SMEM] + [VMEM] * 7,
        out_specs=(VMEM, VMEM),
        scratch_shapes=[pltpu.VMEM((tokens, width), F32), pltpu.VMEM((tokens, 32, 128), BF16)],
        compiler_params=pltpu.CompilerParams(vmem_limit_bytes=14 << 20),
        cost_estimate=pl.CostEstimate(flops=10**9, bytes_accessed=8 * 10**6, transcendentals=0),
        name="mix",
    )(slots, *projected, residual, mixer_gain, expert_gain)


def expert_kernel(
    x_hbm, gate_hbm, up_hbm, down_hbm, o_hbm,
    x_ref, gate_ref, up_ref, down_ref, o_ref, rows_ref, hidden_ref, result_ref, in_sem, out_sem,
):
    sources = x_ref.shape[0]
    slots = x_ref.shape[1] // 32
    gather = to_rows(8, 32)
    spread = to_rows(32, 8)
    weights = ((gate_hbm, gate_ref), (up_hbm, up_ref), (down_hbm, down_ref))

    def slot_copy(source, target, sem, slot):
        at = pl.ds(slot * 32, 32)
        return pltpu.make_async_copy(source.at[:, at, :], target.at[:, at, :], sem.at[slot])

    x_copies = [slot_copy(x_hbm, x_ref, in_sem, slot) for slot in range(slots)]
    w_copies = [
        pltpu.make_async_copy(source, target, in_sem.at[slots + k])
        for k, (source, target) in enumerate(weights)
    ]
    for copy in x_copies + w_copies:
        copy.start()

    for slot in range(slots):
        x_copies[slot].wait()

        @pl.loop(0, sources // 16, unroll=8)
        def _(g):
            at = slice(slot * 32, slot * 32 + 32)
            left = x_ref[pl.ds(g * 16, 8), at, :].reshape(256, 128)
            right = x_ref[pl.ds(g * 16 + 8, 8), at, :].reshape(256, 128)
            got = jnp.dot(
                gather, jnp.concatenate([left, right], axis=1), preferred_element_type=F32
            )
            to = pl.ds(pl.multiple_of(slot * sources + g * 16, 16), 16)
            for c in range(32):
                rows_ref[to, c * 128 : c * 128 + 128] = jnp.concatenate(
                    [got[c * 8 : c * 8 + 8, :128], got[c * 8 : c * 8 + 8, 128:]], axis=0
                ).astype(BF16)

    w_copies[0].wait()
    w_copies[1].wait()
    for n in range(0, 512, 256):
        a = jnp.dot(rows_ref[...], gate_ref[:, n : n + 256], preferred_element_type=F32)
        b = jnp.dot(rows_ref[...], up_ref[:, n : n + 256], preferred_element_type=F32)
        hidden_ref[:, n : n + 256] = (a / (1.0 + jnp.exp(-a)) * b).astype(BF16)

    w_copies[2].wait()
    for n in range(0, 4096, 1024):
        result_ref[:, n : n + 1024] = jnp.dot(
            hidden_ref[...], down_ref[:, n : n + 1024], preferred_element_type=F32
        )

    o_copies = [slot_copy(o_ref, o_hbm, out_sem, slot) for slot in range(slots)]
    for slot in range(slots):

        @pl.loop(0, sources // 16, unroll=8)
        def _(g):
            base = slot * sources + g * 16
            lower = result_ref[pl.ds(pl.multiple_of(base, 8), 8), :]
            upper = result_ref[pl.ds(pl.multiple_of(base + 8, 8), 8), :]
            out = jnp.dot(
                spread, stack_blocks(lower, upper).astype(BF16), preferred_element_type=F32
            ).astype(BF16)
            at = slice(slot * 32, slot * 32 + 32)
            o_ref[pl.ds(g * 16, 8), at, :] = out[:, :128].reshape(8, 32, 128)
            o_ref[pl.ds(g * 16 + 8, 8), at, :] = out[:, 128:].reshape(8, 32, 128)

        o_copies[slot].start()
    for copy in o_copies:
        copy.wait()


def run_experts(x, gate, up, down):
    slots = x.shape[1] // 32
    rows = x.shape[0] * slots
    return pl.pallas_call(
        expert_kernel,
        out_shape=pltpu.HBM(x.shape, BF16),
        in_specs=[HBM] * 4,
        out_specs=HBM,
        scratch_shapes=[
            pltpu.VMEM(x.shape, BF16),
            pltpu.VMEM(gate.shape, BF16),
            pltpu.VMEM(up.shape, BF16),
            pltpu.VMEM(down.shape, BF16),
            pltpu.VMEM(x.shape, BF16),
            pltpu.VMEM((rows, 4096), BF16),
            pltpu.VMEM((rows, 512), BF16),
            pltpu.VMEM((rows, 4096), F32),
            pltpu.SemaphoreType.DMA((slots + 3,)),
            pltpu.SemaphoreType.DMA((slots,)),
        ],
        compiler_params=pltpu.CompilerParams(vmem_limit_bytes=56 << 20),
        cost_estimate=pl.CostEstimate(flops=6 * 10**9, bytes_accessed=19 * 10**6, transcendentals=0),
        name="experts",
    )(x, gate, up, down)


def combine_kernel(expert_ref, rank_ref, weight_ref, x_ref, stream_ref, gain_ref, o_ref, out_ref):
    tokens = stream_ref.shape[0]
    gather = to_rows(8, 32)
    gain = gain_ref[...]

    @pl.loop(0, tokens, unroll=16)
    def _(t):
        total = None
        for k in range(2):
            rank = pl.multiple_of(rank_ref[k, t] * 32, 32)
            part = x_ref[expert_ref[k, t], pl.ds(rank, 32), :].astype(F32) * weight_ref[k, t]
            total = part if total is None else total + part
        square = jnp.sum(jnp.sum(total * total, axis=0, keepdims=True), axis=1, keepdims=True)
        r = lax.rsqrt(square * (1.0 / 4096) + EPSILON)
        out_ref[t] = (stream_ref[t].astype(F32) + total * r * gain).astype(BF16)

    @pl.loop(0, tokens // 16, unroll=8)
    def _(g):
        left = out_ref[pl.ds(g * 16, 8)].reshape(256, 128)
        right = out_ref[pl.ds(g * 16 + 8, 8)].reshape(256, 128)
        got = jnp.dot(gather, jnp.concatenate([left, right], axis=1), preferred_element_type=F32)
        to = pl.ds(pl.multiple_of(g * 16, 16), 16)
        for c in range(32):
            o_ref[to, c * 128 : c * 128 + 128] = jnp.concatenate(
                [got[c * 8 : c * 8 + 8, :128], got[c * 8 : c * 8 + 8, 128:]], axis=0
            ).astype(BF16)


def combine(expert, rank, weight, x, stream, gain):
    tokens = stream.shape[0]
    return pl.pallas_call(
        combine_kernel,
        out_shape=jax.ShapeDtypeStruct((tokens, 4096), BF16),
        in_specs=[SMEM, SMEM, SMEM, VMEM, VMEM, VMEM],
        out_specs=VMEM,
        scratch_shapes=[pltpu.VMEM((tokens, 32, 128), BF16)],
        compiler_params=pltpu.CompilerParams(vmem_limit_bytes=14 << 20),
        cost_estimate=pl.CostEstimate(flops=10**9, bytes_accessed=6 * 10**6, transcendentals=0),
        name="combine",
    )(expert, rank, weight, x, stream, gain)


def layer(
    queries, key_rows, values, residual, out_weight, mixer_gain, expert_gain,
    gate_weight, up_weight, expert_down_matrix, routes, route_weight, output_gain,
):
    onward = [(d, (d + (2, 6)[d % 2]) % 8) for d in range(8)]
    back = [(d, (d + (6, 2)[d % 2]) % 8) for d in range(8)]
    swap = [(0, 1), (1, 0)]
    w_first = lax.ppermute(out_weight, DP, onward)
    w_second = lax.ppermute(out_weight, DP, back)
    w_far = lax.ppermute(w_first, DP, onward)

    picks = jnp.transpose(routes[0])
    rank, slots = route(picks)

    packed = jnp.concatenate(
        [jnp.transpose(a[0], (1, 0, 2)) for a in (queries, key_rows, values)], axis=1
    )
    by_head = lax.all_to_all(packed, "sp", split_axis=0, concat_axis=0, tiled=True)
    attended = attend(by_head)
    own_x = lax.all_to_all(attended, "sp", split_axis=0, concat_axis=0, tiled=True)
    other_x = lax.ppermute(own_x, "c", swap)
    own, other = project(own_x, other_x, (out_weight, w_first, w_second))
    got = lax.ppermute(other, "c", swap)
    own_far, other_far = project(own_x, other_x, (w_far,))
    got_far = lax.ppermute(other_far, "c", swap)
    stream, outgoing = mix(
        slots, (own, own_far, got, got_far), residual[0], mixer_gain.reshape(1, -1),
        expert_gain.reshape(1, -1),
    )
    arrived = lax.all_to_all(outgoing, ALL, split_axis=0, concat_axis=0, tiled=True)
    result = run_experts(arrived, gate_weight[0], up_weight[0], expert_down_matrix[0])
    returned = lax.all_to_all(result, ALL, split_axis=0, concat_axis=0, tiled=True)
    output = combine(
        picks, rank, jnp.transpose(route_weight[0]), returned, stream, output_gain.reshape(32, 128)
    )
    return output[None]


def solution(mesh):
    mesh = Mesh(mesh.devices.reshape(16, 2, 2, 2), ALL)
    in_specs = (
        P(DP, "sp", None, None),
        P(DP, "sp", None, None),
        P(DP, "sp", None, None),
        P(DP, "sp", None),
        P(None, DP),
        P(),
        P(),
        P(ALL, None, None),
        P(ALL, None, None),
        P(ALL, None, None),
        P(DP, "sp", None),
        P(DP, "sp", None),
        P(),
    )
    return jax.shard_map(
        layer, mesh=mesh, in_specs=in_specs, out_specs=P(DP, "sp", None), check_vma=False
    )
```

```python
import math

import jax
import jax.numpy as jnp
from jax import lax
from jax.experimental import pallas as pl
from jax.experimental.pallas import tpu as pltpu
from jax.sharding import Mesh, PartitionSpec as P


EPSILON = 1e-06
F32 = jnp.float32
BF16 = jnp.bfloat16
DP = ("yh", "yl", "c")
ALL = ("sp", "yh", "yl", "c")
VMEM = pl.BlockSpec(memory_space=pltpu.VMEM)
ANY = pl.BlockSpec(memory_space=pl.ANY)
HBM = pl.BlockSpec(memory_space=pltpu.HBM)
SMEM = pl.BlockSpec(memory_space=pltpu.SMEM)


def attend_kernel(x_ref, o_ref):
    blocks, _, hd = x_ref.shape
    tile = 256
    scale = math.log2(math.e) * hd ** -0.5
    row = lax.broadcasted_iota(jnp.int32, (256, 256), 0) % 128
    col = lax.broadcasted_iota(jnp.int32, (256, 256), 1)
    sums = jnp.where((col >= 128) | (row > col), 1.0, 0.0).astype(BF16)
    query_pos = lax.broadcasted_iota(jnp.int32, (tile, 128), 0)
    key_pos = lax.broadcasted_iota(jnp.int32, (tile, 128), 1)

    def two(block, start):
        return jnp.concatenate(
            [x_ref[2 * block, start : start + 128], x_ref[2 * block + 1, start : start + 128]], axis=0
        )

    for i in range(blocks // 2):
        q = two(i, 0)
        carry, total = None, None
        for j in range(i, -1, -1):
            z = (
                lax.dot_general(q, two(j, 128), (((1,), (1,)), ((), ())), preferred_element_type=F32)
                * scale
            )
            weights = [None, None]
            for half in (1, 0):
                zh = z[:, half * 128 : half * 128 + 128]
                keep = jnp.maximum(zh, 0.0) + jnp.log2(1.0 + jnp.exp2(-jnp.abs(zh)))
                take = zh - keep
                if i == j:
                    past = key_pos + half * 128 < query_pos
                    keep = jnp.where(past, keep, 0.0)
                high = keep.astype(BF16)
                low = (keep - high.astype(F32)).astype(BF16)
                s = jnp.dot(jnp.concatenate([high, low], axis=1), sums, preferred_element_type=F32)
                e = take - s[:, :128]
                if carry is not None:
                    e = e - carry
                w = jnp.exp2(e)
                if i == j:
                    w = jnp.where(past, w, 0.0)
                weights[half] = w.astype(BF16)
                carry = s[:, 128:] if carry is None else carry + s[:, 128:]
            part = jnp.dot(
                jnp.concatenate(weights, axis=1), two(j, 256), preferred_element_type=F32
            )
            total = part if total is None else total + part
        total = total.astype(BF16)
        o_ref[2 * i] = total[:128]
        o_ref[2 * i + 1] = total[128:]


def attend(x):
    blocks = x.shape[0]
    return pl.pallas_call(
        attend_kernel,
        out_shape=jax.ShapeDtypeStruct((blocks, 128, 128), BF16),
        in_specs=[VMEM],
        out_specs=VMEM,
        compiler_params=pltpu.CompilerParams(vmem_limit_bytes=14 << 20),
        cost_estimate=pl.CostEstimate(
            flops=12 * 10**9, bytes_accessed=3 * 10**6, transcendentals=7 * 10**6
        ),
        name="attend",
    )(x)


def route_kernel(picks_ref, rank_ref, slot_ref):
    tokens = picks_ref.shape[1]
    experts = 128
    expert = lax.broadcasted_iota(jnp.int32, (experts, tokens), 0)
    one, zero = jnp.ones((), F32), jnp.zeros((), F32)
    earlier = jnp.where(
        lax.broadcasted_iota(jnp.int32, (tokens, tokens), 0)
        < lax.broadcasted_iota(jnp.int32, (tokens, tokens), 1),
        one, zero,
    ).astype(BF16)
    number = lax.broadcasted_iota(jnp.int32, (1, tokens), 1).astype(F32)
    taken, slots = None, None
    for k in range(picks_ref.shape[0]):
        onehot = jnp.where(expert == picks_ref[k : k + 1, :], one, zero)
        before = jnp.dot(onehot.astype(BF16), earlier, preferred_element_type=F32)
        if taken is not None:
            before = before + taken
        rank = jnp.sum(onehot * before, axis=0, keepdims=True)
        count = jnp.sum(onehot, axis=1, keepdims=True)
        taken = count if taken is None else taken + count
        rank_ref[k : k + 1, :] = rank.astype(jnp.int32)
        slot = lax.broadcasted_iota(jnp.int32, (8, tokens), 0).astype(F32)
        held = jnp.where(slot == rank, number, zero).astype(BF16)
        part = lax.dot_general(
            held, onehot.astype(BF16), (((1,), (1,)), ((), ())), preferred_element_type=F32
        )
        slots = part if slots is None else slots + part
    slot_ref[...] = slots.astype(jnp.int32)


def route(picks):
    return pl.pallas_call(
        route_kernel,
        out_shape=(
            jax.ShapeDtypeStruct(picks.shape, jnp.int32),
            jax.ShapeDtypeStruct((8, 128), jnp.int32),
        ),
        in_specs=[VMEM],
        out_specs=(VMEM, VMEM),
        compiler_params=pltpu.CompilerParams(vmem_limit_bytes=4 << 20),
        cost_estimate=pl.CostEstimate(flops=2 * 10**7, bytes_accessed=10**4, transcendentals=0),
        name="route",
    )(picks)


def project_kernel(own_x_ref, other_x_ref, *refs):
    *weights, own_ref, other_ref, w_ref, sem = refs
    copies = [
        pltpu.make_async_copy(ref, w_ref.at[k], sem.at[k]) for k, ref in enumerate(weights)
    ]
    for copy in copies:
        copy.start()
    heads = own_x_ref.shape[0]
    rows = [
        jnp.concatenate([ref[h] for h in range(heads)], axis=1) for ref in (own_x_ref, other_x_ref)
    ]
    both = jnp.concatenate(rows, axis=0)
    for k, copy in enumerate(copies):
        copy.wait()
        for n in range(0, 512, 256):
            out = jnp.dot(both, w_ref[k, :, n : n + 256], preferred_element_type=F32)
            own_ref[k, :, n : n + 256] = out[:128]
            other_ref[k, :, n : n + 256] = out[128:]


def project(own_x, other_x, weights):
    count = len(weights)
    shape = jax.ShapeDtypeStruct((count, 128, 512), F32)
    return pl.pallas_call(
        project_kernel,
        out_shape=(shape, shape),
        in_specs=[VMEM, VMEM] + [ANY] * count,
        out_specs=(VMEM, VMEM),
        scratch_shapes=[
            pltpu.VMEM((count, 2048, 512), BF16),
            pltpu.SemaphoreType.DMA((count,)),
        ],
        compiler_params=pltpu.CompilerParams(vmem_limit_bytes=(5 + 3 * count) << 20),
        cost_estimate=pl.CostEstimate(
            flops=count * 10**9, bytes_accessed=count * 3 * 10**6, transcendentals=0
        ),
    )(own_x, other_x, *weights)


def to_rows(inner, outer):
    i = lax.broadcasted_iota(jnp.int32, (256, 256), 0)
    k = lax.broadcasted_iota(jnp.int32, (256, 256), 1)
    return jnp.where(k == (i % inner) * outer + i // inner, 1.0, 0.0).astype(BF16)


def stack_blocks(lower, upper):
    left = jnp.concatenate([lower[:, c * 128 : c * 128 + 128] for c in range(32)], axis=0)
    right = jnp.concatenate([upper[:, c * 128 : c * 128 + 128] for c in range(32)], axis=0)
    return jnp.concatenate([left, right], axis=1)


def mix_kernel(
    slot_ref, own_ref, own_far_ref, got_ref, got_far_ref, residual_ref, mixer_ref, expert_ref,
    stream_ref, out_ref, proj_ref, rows_ref,
):
    chip, core = lax.axis_index("yh") * 2 + lax.axis_index("yl"), lax.axis_index("c")
    for member, near, far in ((core, own_ref, own_far_ref), (1 - core, got_ref, got_far_ref)):
        for k, step in enumerate((0, 3 - 2 * member, 1 + 2 * member, 2)):
            at = lax.rem(chip + step, 4) * 1024 + member * 512
            block = near[k] if k < 3 else far[0]
            proj_ref[:, pl.ds(pl.multiple_of(at, 512), 512)] = block
    spread = to_rows(32, 8)
    width = proj_ref.shape[1]

    @pl.loop(0, proj_ref.shape[0] // 16, unroll=8)
    def _(g):
        at = pl.ds(pl.multiple_of(g * 16, 16), 16)
        p = proj_ref[at, :]
        r = lax.rsqrt(jnp.sum(p * p, axis=1, keepdims=True) * (1.0 / width) + EPSILON)
        stream = (residual_ref[at, :].astype(F32) + p * r * mixer_ref[...]).astype(BF16)
        s = stream.astype(F32)
        r = lax.rsqrt(jnp.sum(s * s, axis=1, keepdims=True) * (1.0 / width) + EPSILON)
        x = s * r * expert_ref[...]
        for value, ref in ((s, stream_ref), (x, rows_ref)):
            spread_out = jnp.dot(
                spread, stack_blocks(value[:8], value[8:]).astype(BF16), preferred_element_type=F32
            ).astype(BF16)
            ref[pl.ds(g * 16, 8)] = spread_out[:, :128].reshape(8, 32, 128)
            ref[pl.ds(g * 16 + 8, 8)] = spread_out[:, 128:].reshape(8, 32, 128)

    experts = out_ref.shape[0]

    @pl.loop(0, experts, unroll=16)
    def _(e):
        for slot in range(out_ref.shape[1] // 32):
            out_ref[e, slot * 32 : slot * 32 + 32, :] = rows_ref[slot_ref[slot, e]]


def mix(slots, projected, residual, mixer_gain, expert_gain):
    tokens, width = residual.shape
    return pl.pallas_call(
        mix_kernel,
        out_shape=(
            jax.ShapeDtypeStruct((tokens, 32, 128), BF16),
            jax.ShapeDtypeStruct((128, 96, 128), BF16),
        ),
        in_specs=[SMEM] + [VMEM] * 7,
        out_specs=(VMEM, VMEM),
        scratch_shapes=[pltpu.VMEM((tokens, width), F32), pltpu.VMEM((tokens, 32, 128), BF16)],
        compiler_params=pltpu.CompilerParams(vmem_limit_bytes=14 << 20),
        cost_estimate=pl.CostEstimate(flops=10**9, bytes_accessed=8 * 10**6, transcendentals=0),
        name="mix",
    )(slots, *projected, residual, mixer_gain, expert_gain)


def expert_kernel(x_ref, gate_ref, up_ref, down_ref, o_ref, rows_ref, hidden_ref, result_ref):
    sources = x_ref.shape[0]
    slots = x_ref.shape[1] // 32
    gather = to_rows(8, 32)
    spread = to_rows(32, 8)

    for slot in range(slots):

        @pl.loop(0, sources // 16, unroll=8)
        def _(g):
            at = slice(slot * 32, slot * 32 + 32)
            left = x_ref[pl.ds(g * 16, 8), at, :].reshape(256, 128)
            right = x_ref[pl.ds(g * 16 + 8, 8), at, :].reshape(256, 128)
            got = jnp.dot(
                gather, jnp.concatenate([left, right], axis=1), preferred_element_type=F32
            )
            to = pl.ds(pl.multiple_of(slot * sources + g * 16, 16), 16)
            for c in range(32):
                rows_ref[to, c * 128 : c * 128 + 128] = jnp.concatenate(
                    [got[c * 8 : c * 8 + 8, :128], got[c * 8 : c * 8 + 8, 128:]], axis=0
                ).astype(BF16)

    for n in range(0, 512, 256):
        a = jnp.dot(rows_ref[...], gate_ref[:, n : n + 256], preferred_element_type=F32)
        b = jnp.dot(rows_ref[...], up_ref[:, n : n + 256], preferred_element_type=F32)
        hidden_ref[:, n : n + 256] = (a / (1.0 + jnp.exp(-a)) * b).astype(BF16)

    for n in range(0, 4096, 1024):
        result_ref[:, n : n + 1024] = jnp.dot(
            hidden_ref[...], down_ref[:, n : n + 1024], preferred_element_type=F32
        )

    for slot in range(slots):

        @pl.loop(0, sources // 16, unroll=8)
        def _(g):
            base = slot * sources + g * 16
            lower = result_ref[pl.ds(pl.multiple_of(base, 8), 8), :]
            upper = result_ref[pl.ds(pl.multiple_of(base + 8, 8), 8), :]
            out = jnp.dot(
                spread, stack_blocks(lower, upper).astype(BF16), preferred_element_type=F32
            ).astype(BF16)
            at = slice(slot * 32, slot * 32 + 32)
            o_ref[pl.ds(g * 16, 8), at, :] = out[:, :128].reshape(8, 32, 128)
            o_ref[pl.ds(g * 16 + 8, 8), at, :] = out[:, 128:].reshape(8, 32, 128)


def run_experts(x, gate, up, down):
    rows = x.shape[0] * (x.shape[1] // 32)
    return pl.pallas_call(
        expert_kernel,
        out_shape=jax.ShapeDtypeStruct(x.shape, BF16),
        in_specs=[VMEM] * 4,
        out_specs=VMEM,
        scratch_shapes=[
            pltpu.VMEM((rows, 4096), BF16),
            pltpu.VMEM((rows, 512), BF16),
            pltpu.VMEM((rows, 4096), F32),
        ],
        compiler_params=pltpu.CompilerParams(vmem_limit_bytes=18 << 20),
        cost_estimate=pl.CostEstimate(flops=6 * 10**9, bytes_accessed=19 * 10**6, transcendentals=0),
        name="experts",
    )(x, gate, up, down)


def combine_kernel(expert_ref, rank_ref, weight_ref, x_ref, stream_ref, gain_ref, o_ref, out_ref):
    tokens = stream_ref.shape[0]
    gather = to_rows(8, 32)
    gain = gain_ref[...]

    @pl.loop(0, tokens, unroll=16)
    def _(t):
        total = None
        for k in range(2):
            rank = pl.multiple_of(rank_ref[k, t] * 32, 32)
            part = x_ref[expert_ref[k, t], pl.ds(rank, 32), :].astype(F32) * weight_ref[k, t]
            total = part if total is None else total + part
        square = jnp.sum(jnp.sum(total * total, axis=0, keepdims=True), axis=1, keepdims=True)
        r = lax.rsqrt(square * (1.0 / 4096) + EPSILON)
        out_ref[t] = (stream_ref[t].astype(F32) + total * r * gain).astype(BF16)

    @pl.loop(0, tokens // 16, unroll=8)
    def _(g):
        left = out_ref[pl.ds(g * 16, 8)].reshape(256, 128)
        right = out_ref[pl.ds(g * 16 + 8, 8)].reshape(256, 128)
        got = jnp.dot(gather, jnp.concatenate([left, right], axis=1), preferred_element_type=F32)
        to = pl.ds(pl.multiple_of(g * 16, 16), 16)
        for c in range(32):
            o_ref[to, c * 128 : c * 128 + 128] = jnp.concatenate(
                [got[c * 8 : c * 8 + 8, :128], got[c * 8 : c * 8 + 8, 128:]], axis=0
            ).astype(BF16)


def combine(expert, rank, weight, x, stream, gain):
    tokens = stream.shape[0]
    return pl.pallas_call(
        combine_kernel,
        out_shape=jax.ShapeDtypeStruct((tokens, 4096), BF16),
        in_specs=[SMEM, SMEM, SMEM, VMEM, VMEM, VMEM],
        out_specs=VMEM,
        scratch_shapes=[pltpu.VMEM((tokens, 32, 128), BF16)],
        compiler_params=pltpu.CompilerParams(vmem_limit_bytes=14 << 20),
        cost_estimate=pl.CostEstimate(flops=10**9, bytes_accessed=6 * 10**6, transcendentals=0),
        name="combine",
    )(expert, rank, weight, x, stream, gain)


def layer(
    queries, key_rows, values, residual, out_weight, mixer_gain, expert_gain,
    gate_weight, up_weight, expert_down_matrix, routes, route_weight, output_gain,
):
    onward = [(d, (d + (2, 6)[d % 2]) % 8) for d in range(8)]
    back = [(d, (d + (6, 2)[d % 2]) % 8) for d in range(8)]
    swap = [(0, 1), (1, 0)]
    w_first = lax.ppermute(out_weight, DP, onward)
    w_second = lax.ppermute(out_weight, DP, back)
    w_far = lax.ppermute(w_first, DP, onward)

    picks = jnp.transpose(routes[0])
    rank, slots = route(picks)

    packed = jnp.concatenate(
        [jnp.transpose(a[0], (1, 0, 2)) for a in (queries, key_rows, values)], axis=1
    )
    by_head = lax.all_to_all(packed, "sp", split_axis=0, concat_axis=0, tiled=True)
    attended = attend(by_head)
    own_x = lax.all_to_all(attended, "sp", split_axis=0, concat_axis=0, tiled=True)
    other_x = lax.ppermute(own_x, "c", swap)
    own, other = project(own_x, other_x, (out_weight, w_first, w_second))
    got = lax.ppermute(other, "c", swap)
    own_far, other_far = project(own_x, other_x, (w_far,))
    got_far = lax.ppermute(other_far, "c", swap)
    stream, outgoing = mix(
        slots, (own, own_far, got, got_far), residual[0], mixer_gain.reshape(1, -1),
        expert_gain.reshape(1, -1),
    )
    arrived = lax.all_to_all(outgoing, ALL, split_axis=0, concat_axis=0, tiled=True)
    result = run_experts(arrived, gate_weight[0], up_weight[0], expert_down_matrix[0])
    returned = lax.all_to_all(result, ALL, split_axis=0, concat_axis=0, tiled=True)
    output = combine(
        picks, rank, jnp.transpose(route_weight[0]), returned, stream, output_gain.reshape(32, 128)
    )
    return output[None]


def solution(mesh):
    mesh = Mesh(mesh.devices.reshape(16, 2, 2, 2), ALL)
    in_specs = (
        P(DP, "sp", None, None),
        P(DP, "sp", None, None),
        P(DP, "sp", None, None),
        P(DP, "sp", None),
        P(None, DP),
        P(),
        P(),
        P(ALL, None, None),
        P(ALL, None, None),
        P(ALL, None, None),
        P(DP, "sp", None),
        P(DP, "sp", None),
        P(),
    )
    return jax.shard_map(
        layer, mesh=mesh, in_specs=in_specs, out_specs=P(DP, "sp", None), check_vma=False
    )
```

```python
import math

import jax
import jax.numpy as jnp
from jax import lax
from jax.experimental import pallas as pl
from jax.experimental.pallas import tpu as pltpu
from jax.sharding import Mesh, PartitionSpec as P


EPSILON = 1e-06
F32 = jnp.float32
BF16 = jnp.bfloat16
DP = ("yh", "yl", "c")
ALL = ("sp", "yh", "yl", "c")
VMEM = pl.BlockSpec(memory_space=pltpu.VMEM)
ANY = pl.BlockSpec(memory_space=pl.ANY)
HBM = pl.BlockSpec(memory_space=pltpu.HBM)
CHUNKS = 4
SMEM = pl.BlockSpec(memory_space=pltpu.SMEM)


def attend_kernel(x_ref, o_ref):
    blocks, _, hd = x_ref.shape
    tile = 256
    scale = math.log2(math.e) * hd ** -0.5
    row = lax.broadcasted_iota(jnp.int32, (256, 256), 0) % 128
    col = lax.broadcasted_iota(jnp.int32, (256, 256), 1)
    sums = jnp.where((col >= 128) | (row > col), 1.0, 0.0).astype(BF16)
    query_pos = lax.broadcasted_iota(jnp.int32, (tile, 128), 0)
    key_pos = lax.broadcasted_iota(jnp.int32, (tile, 128), 1)

    def two(block, start):
        return jnp.concatenate(
            [x_ref[2 * block, start : start + 128], x_ref[2 * block + 1, start : start + 128]], axis=0
        )

    for i in range(blocks // 2):
        q = two(i, 0)
        carry, total = None, None
        for j in range(i, -1, -1):
            z = (
                lax.dot_general(q, two(j, 128), (((1,), (1,)), ((), ())), preferred_element_type=F32)
                * scale
            )
            weights = [None, None]
            for half in (1, 0):
                zh = z[:, half * 128 : half * 128 + 128]
                keep = jnp.maximum(zh, 0.0) + jnp.log2(1.0 + jnp.exp2(-jnp.abs(zh)))
                take = zh - keep
                if i == j:
                    past = key_pos + half * 128 < query_pos
                    keep = jnp.where(past, keep, 0.0)
                high = keep.astype(BF16)
                low = (keep - high.astype(F32)).astype(BF16)
                s = jnp.dot(jnp.concatenate([high, low], axis=1), sums, preferred_element_type=F32)
                e = take - s[:, :128]
                if carry is not None:
                    e = e - carry
                w = jnp.exp2(e)
                if i == j:
                    w = jnp.where(past, w, 0.0)
                weights[half] = w.astype(BF16)
                carry = s[:, 128:] if carry is None else carry + s[:, 128:]
            part = jnp.dot(
                jnp.concatenate(weights, axis=1), two(j, 256), preferred_element_type=F32
            )
            total = part if total is None else total + part
        total = total.astype(BF16)
        o_ref[2 * i] = total[:128]
        o_ref[2 * i + 1] = total[128:]


def attend(x):
    blocks = x.shape[0]
    return pl.pallas_call(
        attend_kernel,
        out_shape=jax.ShapeDtypeStruct((blocks, 128, 128), BF16),
        in_specs=[VMEM],
        out_specs=VMEM,
        compiler_params=pltpu.CompilerParams(vmem_limit_bytes=14 << 20),
        cost_estimate=pl.CostEstimate(
            flops=12 * 10**9, bytes_accessed=3 * 10**6, transcendentals=7 * 10**6
        ),
        name="attend",
    )(x)


def route_kernel(picks_ref, rank_ref, slot_ref):
    tokens = picks_ref.shape[1]
    experts = 128
    expert = lax.broadcasted_iota(jnp.int32, (experts, tokens), 0)
    one, zero = jnp.ones((), F32), jnp.zeros((), F32)
    earlier = jnp.where(
        lax.broadcasted_iota(jnp.int32, (tokens, tokens), 0)
        < lax.broadcasted_iota(jnp.int32, (tokens, tokens), 1),
        one, zero,
    ).astype(BF16)
    number = lax.broadcasted_iota(jnp.int32, (1, tokens), 1).astype(F32)
    taken, slots = None, None
    for k in range(picks_ref.shape[0]):
        onehot = jnp.where(expert == picks_ref[k : k + 1, :], one, zero)
        before = jnp.dot(onehot.astype(BF16), earlier, preferred_element_type=F32)
        if taken is not None:
            before = before + taken
        rank = jnp.sum(onehot * before, axis=0, keepdims=True)
        count = jnp.sum(onehot, axis=1, keepdims=True)
        taken = count if taken is None else taken + count
        rank_ref[k : k + 1, :] = rank.astype(jnp.int32)
        slot = lax.broadcasted_iota(jnp.int32, (8, tokens), 0).astype(F32)
        held = jnp.where(slot == rank, number, zero).astype(BF16)
        part = lax.dot_general(
            held, onehot.astype(BF16), (((1,), (1,)), ((), ())), preferred_element_type=F32
        )
        slots = part if slots is None else slots + part
    slot_ref[...] = slots.astype(jnp.int32)


def route(picks):
    return pl.pallas_call(
        route_kernel,
        out_shape=(
            jax.ShapeDtypeStruct(picks.shape, jnp.int32),
            jax.ShapeDtypeStruct((8, 128), jnp.int32),
        ),
        in_specs=[VMEM],
        out_specs=(VMEM, VMEM),
        compiler_params=pltpu.CompilerParams(vmem_limit_bytes=4 << 20),
        cost_estimate=pl.CostEstimate(flops=2 * 10**7, bytes_accessed=10**4, transcendentals=0),
        name="route",
    )(picks)


def project_kernel(own_x_ref, other_x_ref, *refs):
    *weights, own_ref, other_ref, w_ref, sem = refs
    copies = [
        pltpu.make_async_copy(ref, w_ref.at[k], sem.at[k]) for k, ref in enumerate(weights)
    ]
    for copy in copies:
        copy.start()
    heads = own_x_ref.shape[0]
    rows = [
        jnp.concatenate([ref[h] for h in range(heads)], axis=1) for ref in (own_x_ref, other_x_ref)
    ]
    both = jnp.concatenate(rows, axis=0)
    for k, copy in enumerate(copies):
        copy.wait()
        for n in range(0, 512, 256):
            out = jnp.dot(both, w_ref[k, :, n : n + 256], preferred_element_type=F32)
            own_ref[k, :, n : n + 256] = out[:128]
            other_ref[k, :, n : n + 256] = out[128:]


def project(own_x, other_x, weights):
    count = len(weights)
    shape = jax.ShapeDtypeStruct((count, 128, 512), F32)
    return pl.pallas_call(
        project_kernel,
        out_shape=(shape, shape),
        in_specs=[VMEM, VMEM] + [ANY] * count,
        out_specs=(VMEM, VMEM),
        scratch_shapes=[
            pltpu.VMEM((count, 2048, 512), BF16),
            pltpu.SemaphoreType.DMA((count,)),
        ],
        compiler_params=pltpu.CompilerParams(vmem_limit_bytes=(5 + 3 * count) << 20),
        cost_estimate=pl.CostEstimate(
            flops=count * 10**9, bytes_accessed=count * 3 * 10**6, transcendentals=0
        ),
    )(own_x, other_x, *weights)


def to_rows(inner, outer):
    i = lax.broadcasted_iota(jnp.int32, (256, 256), 0)
    k = lax.broadcasted_iota(jnp.int32, (256, 256), 1)
    return jnp.where(k == (i % inner) * outer + i // inner, 1.0, 0.0).astype(BF16)


def stack_blocks(lower, upper):
    left = jnp.concatenate([lower[:, c * 128 : c * 128 + 128] for c in range(32)], axis=0)
    right = jnp.concatenate([upper[:, c * 128 : c * 128 + 128] for c in range(32)], axis=0)
    return jnp.concatenate([left, right], axis=1)


def mix_kernel(
    slot_ref, own_ref, own_far_ref, got_ref, got_far_ref, residual_ref, mixer_ref, expert_ref,
    stream_ref, out_ref, proj_ref, rows_ref,
):
    chip, core = lax.axis_index("yh") * 2 + lax.axis_index("yl"), lax.axis_index("c")
    for member, near, far in ((core, own_ref, own_far_ref), (1 - core, got_ref, got_far_ref)):
        for k, step in enumerate((0, 3 - 2 * member, 1 + 2 * member, 2)):
            at = lax.rem(chip + step, 4) * 1024 + member * 512
            block = near[k] if k < 3 else far[0]
            proj_ref[:, pl.ds(pl.multiple_of(at, 512), 512)] = block
    spread = to_rows(32, 8)
    width = proj_ref.shape[1]

    @pl.loop(0, proj_ref.shape[0] // 16, unroll=8)
    def _(g):
        at = pl.ds(pl.multiple_of(g * 16, 16), 16)
        p = proj_ref[at, :]
        r = lax.rsqrt(jnp.sum(p * p, axis=1, keepdims=True) * (1.0 / width) + EPSILON)
        stream = (residual_ref[at, :].astype(F32) + p * r * mixer_ref[...]).astype(BF16)
        s = stream.astype(F32)
        r = lax.rsqrt(jnp.sum(s * s, axis=1, keepdims=True) * (1.0 / width) + EPSILON)
        x = s * r * expert_ref[...]
        for value, ref in ((s, stream_ref), (x, rows_ref)):
            spread_out = jnp.dot(
                spread, stack_blocks(value[:8], value[8:]).astype(BF16), preferred_element_type=F32
            ).astype(BF16)
            ref[pl.ds(g * 16, 8)] = spread_out[:, :128].reshape(8, 32, 128)
            ref[pl.ds(g * 16 + 8, 8)] = spread_out[:, 128:].reshape(8, 32, 128)

    experts = out_ref.shape[0]

    @pl.loop(0, experts, unroll=16)
    def _(e):
        for slot in range(out_ref.shape[1] // 32):
            out_ref[e, slot * 32 : slot * 32 + 32, :] = rows_ref[slot_ref[slot, e]]


def mix(slots, projected, residual, mixer_gain, expert_gain):
    tokens, width = residual.shape
    return pl.pallas_call(
        mix_kernel,
        out_shape=(
            jax.ShapeDtypeStruct((tokens, 32, 128), BF16),
            jax.ShapeDtypeStruct((128, 96, 128), BF16),
        ),
        in_specs=[SMEM] + [VMEM] * 7,
        out_specs=(VMEM, VMEM),
        scratch_shapes=[pltpu.VMEM((tokens, width), F32), pltpu.VMEM((tokens, 32, 128), BF16)],
        compiler_params=pltpu.CompilerParams(vmem_limit_bytes=14 << 20),
        cost_estimate=pl.CostEstimate(flops=10**9, bytes_accessed=8 * 10**6, transcendentals=0),
        name="mix",
    )(slots, *projected, residual, mixer_gain, expert_gain)


def expert_kernel(x_ref, gate_ref, up_ref, down_ref, o_ref, rows_ref, hidden_ref, result_ref):
    sources = x_ref.shape[0]
    slots = x_ref.shape[1] // 32
    gather = to_rows(8, 32)
    spread = to_rows(32, 8)

    for slot in range(slots):

        @pl.loop(0, sources // 16, unroll=8)
        def _(g):
            at = slice(slot * 32, slot * 32 + 32)
            left = x_ref[pl.ds(g * 16, 8), at, :].reshape(256, 128)
            right = x_ref[pl.ds(g * 16 + 8, 8), at, :].reshape(256, 128)
            got = jnp.dot(
                gather, jnp.concatenate([left, right], axis=1), preferred_element_type=F32
            )
            to = pl.ds(pl.multiple_of(slot * sources + g * 16, 16), 16)
            for c in range(32):
                rows_ref[to, c * 128 : c * 128 + 128] = jnp.concatenate(
                    [got[c * 8 : c * 8 + 8, :128], got[c * 8 : c * 8 + 8, 128:]], axis=0
                ).astype(BF16)

    for n in range(0, 512, 256):
        a = jnp.dot(rows_ref[...], gate_ref[:, n : n + 256], preferred_element_type=F32)
        b = jnp.dot(rows_ref[...], up_ref[:, n : n + 256], preferred_element_type=F32)
        hidden_ref[:, n : n + 256] = (a / (1.0 + jnp.exp(-a)) * b).astype(BF16)

    for n in range(0, 4096, 1024):
        result_ref[:, n : n + 1024] = jnp.dot(
            hidden_ref[...], down_ref[:, n : n + 1024], preferred_element_type=F32
        )

    for slot in range(slots):

        @pl.loop(0, sources // 16, unroll=8)
        def _(g):
            base = slot * sources + g * 16
            lower = result_ref[pl.ds(pl.multiple_of(base, 8), 8), :]
            upper = result_ref[pl.ds(pl.multiple_of(base + 8, 8), 8), :]
            out = jnp.dot(
                spread, stack_blocks(lower, upper).astype(BF16), preferred_element_type=F32
            ).astype(BF16)
            at = slice(slot * 32, slot * 32 + 32)
            o_ref[pl.ds(g * 16, 8), at, :] = out[:, :128].reshape(8, 32, 128)
            o_ref[pl.ds(g * 16 + 8, 8), at, :] = out[:, 128:].reshape(8, 32, 128)


def run_experts(x, gate, up, down):
    rows = x.shape[0] * (x.shape[1] // 32)
    return pl.pallas_call(
        expert_kernel,
        out_shape=jax.ShapeDtypeStruct(x.shape, BF16),
        in_specs=[VMEM] * 4,
        out_specs=VMEM,
        scratch_shapes=[
            pltpu.VMEM((rows, 4096), BF16),
            pltpu.VMEM((rows, 512), BF16),
            pltpu.VMEM((rows, 4096), F32),
        ],
        compiler_params=pltpu.CompilerParams(vmem_limit_bytes=18 << 20),
        cost_estimate=pl.CostEstimate(flops=6 * 10**9, bytes_accessed=19 * 10**6, transcendentals=0),
        name="experts",
    )(x, gate, up, down)


def combine_kernel(
    expert_ref, rank_ref, weight_ref, x_ref, stream_ref, gain_ref, o_hbm, o_ref, sem
):
    tokens = stream_ref.shape[0]
    gather = to_rows(8, 32)
    gain = gain_ref[...]

    def one(t):
        total = None
        for k in range(2):
            rank = pl.multiple_of(rank_ref[k, t] * 32, 32)
            part = x_ref[expert_ref[k, t], pl.ds(rank, 32), :].astype(F32) * weight_ref[k, t]
            total = part if total is None else total + part
        square = jnp.sum(jnp.sum(total * total, axis=0, keepdims=True), axis=1, keepdims=True)
        r = lax.rsqrt(square * (1.0 / 4096) + EPSILON)
        return (stream_ref[t].astype(F32) + total * r * gain).astype(BF16)

    copies = []
    for chunk in range(CHUNKS):
        size = tokens // CHUNKS

        @pl.loop(0, size // 16, unroll=size // 16)
        def _(g):
            start = chunk * size + g * 16
            left = jnp.concatenate([one(start + t) for t in range(8)], axis=0)
            right = jnp.concatenate([one(start + 8 + t) for t in range(8)], axis=0)
            got = jnp.dot(gather, jnp.concatenate([left, right], axis=1), preferred_element_type=F32)
            to = pl.ds(pl.multiple_of(start, 16), 16)
            for c in range(32):
                o_ref[to, c * 128 : c * 128 + 128] = jnp.concatenate(
                    [got[c * 8 : c * 8 + 8, :128], got[c * 8 : c * 8 + 8, 128:]], axis=0
                ).astype(BF16)

        at = pl.ds(chunk * size, size)
        copy = pltpu.make_async_copy(o_ref.at[at, :], o_hbm.at[at, :], sem.at[chunk])
        copy.start()
        copies.append(copy)
    for copy in copies:
        copy.wait()


def combine(expert, rank, weight, x, stream, gain):
    tokens = stream.shape[0]
    return pl.pallas_call(
        combine_kernel,
        out_shape=jax.ShapeDtypeStruct((tokens, 4096), BF16),
        in_specs=[SMEM, SMEM, SMEM, VMEM, VMEM, VMEM],
        out_specs=pl.BlockSpec(memory_space=pl.ANY),
        scratch_shapes=[pltpu.VMEM((tokens, 4096), BF16), pltpu.SemaphoreType.DMA((CHUNKS,))],
        compiler_params=pltpu.CompilerParams(vmem_limit_bytes=14 << 20),
        cost_estimate=pl.CostEstimate(flops=10**9, bytes_accessed=6 * 10**6, transcendentals=0),
        name="combine",
    )(expert, rank, weight, x, stream, gain)


def layer(
    queries, key_rows, values, residual, out_weight, mixer_gain, expert_gain,
    gate_weight, up_weight, expert_down_matrix, routes, route_weight, output_gain,
):
    onward = [(d, (d + (2, 6)[d % 2]) % 8) for d in range(8)]
    back = [(d, (d + (6, 2)[d % 2]) % 8) for d in range(8)]
    swap = [(0, 1), (1, 0)]
    w_first = lax.ppermute(out_weight, DP, onward)
    w_second = lax.ppermute(out_weight, DP, back)
    w_far = lax.ppermute(w_first, DP, onward)

    picks = jnp.transpose(routes[0])
    rank, slots = route(picks)

    packed = jnp.concatenate(
        [jnp.transpose(a[0], (1, 0, 2)) for a in (queries, key_rows, values)], axis=1
    )
    by_head = lax.all_to_all(packed, "sp", split_axis=0, concat_axis=0, tiled=True)
    attended = attend(by_head)
    own_x = lax.all_to_all(attended, "sp", split_axis=0, concat_axis=0, tiled=True)
    other_x = lax.ppermute(own_x, "c", swap)
    own, other = project(own_x, other_x, (out_weight, w_first, w_second))
    got = lax.ppermute(other, "c", swap)
    own_far, other_far = project(own_x, other_x, (w_far,))
    got_far = lax.ppermute(other_far, "c", swap)
    stream, outgoing = mix(
        slots, (own, own_far, got, got_far), residual[0], mixer_gain.reshape(1, -1),
        expert_gain.reshape(1, -1),
    )
    arrived = lax.all_to_all(outgoing, ALL, split_axis=0, concat_axis=0, tiled=True)
    result = run_experts(arrived, gate_weight[0], up_weight[0], expert_down_matrix[0])
    returned = lax.all_to_all(result, ALL, split_axis=0, concat_axis=0, tiled=True)
    output = combine(
        picks, rank, jnp.transpose(route_weight[0]), returned, stream, output_gain.reshape(32, 128)
    )
    return output[None]


def solution(mesh):
    mesh = Mesh(mesh.devices.reshape(16, 2, 2, 2), ALL)
    in_specs = (
        P(DP, "sp", None, None),
        P(DP, "sp", None, None),
        P(DP, "sp", None, None),
        P(DP, "sp", None),
        P(None, DP),
        P(),
        P(),
        P(ALL, None, None),
        P(ALL, None, None),
        P(ALL, None, None),
        P(DP, "sp", None),
        P(DP, "sp", None),
        P(),
    )
    return jax.shard_map(
        layer, mesh=mesh, in_specs=in_specs, out_specs=P(DP, "sp", None), check_vma=False
    )
```

```python
import functools
import math

import jax
import jax.numpy as jnp
from jax import lax
from jax.experimental import pallas as pl
from jax.experimental.pallas import tpu as pltpu
from jax.sharding import Mesh, PartitionSpec as P


EPSILON = 1e-06
F32 = jnp.float32
BF16 = jnp.bfloat16
DP = ("yh", "yl", "c")
ALL = ("sp", "yh", "yl", "c")
VMEM = pl.BlockSpec(memory_space=pltpu.VMEM)
ANY = pl.BlockSpec(memory_space=pl.ANY)
HBM = pl.BlockSpec(memory_space=pltpu.HBM)
CHUNKS = 4
SMEM = pl.BlockSpec(memory_space=pltpu.SMEM)


def attend_kernel(x_ref, o_ref):
    blocks, _, hd = x_ref.shape
    tile = 256
    scale = math.log2(math.e) * hd ** -0.5
    row = lax.broadcasted_iota(jnp.int32, (256, 256), 0) % 128
    col = lax.broadcasted_iota(jnp.int32, (256, 256), 1)
    sums = jnp.where((col >= 128) | (row > col), 1.0, 0.0).astype(BF16)
    query_pos = lax.broadcasted_iota(jnp.int32, (tile, 128), 0)
    key_pos = lax.broadcasted_iota(jnp.int32, (tile, 128), 1)

    def two(block, start):
        return jnp.concatenate(
            [x_ref[2 * block, start : start + 128], x_ref[2 * block + 1, start : start + 128]], axis=0
        )

    for i in range(blocks // 2):
        q = two(i, 0)
        carry, total = None, None
        for j in range(i, -1, -1):
            z = (
                lax.dot_general(q, two(j, 128), (((1,), (1,)), ((), ())), preferred_element_type=F32)
                * scale
            )
            weights = [None, None]
            for half in (1, 0):
                zh = z[:, half * 128 : half * 128 + 128]
                keep = jnp.maximum(zh, 0.0) + jnp.log2(1.0 + jnp.exp2(-jnp.abs(zh)))
                take = zh - keep
                if i == j:
                    past = key_pos + half * 128 < query_pos
                    keep = jnp.where(past, keep, 0.0)
                high = keep.astype(BF16)
                low = (keep - high.astype(F32)).astype(BF16)
                s = jnp.dot(jnp.concatenate([high, low], axis=1), sums, preferred_element_type=F32)
                e = take - s[:, :128]
                if carry is not None:
                    e = e - carry
                w = jnp.exp2(e)
                if i == j:
                    w = jnp.where(past, w, 0.0)
                weights[half] = w.astype(BF16)
                carry = s[:, 128:] if carry is None else carry + s[:, 128:]
            part = jnp.dot(
                jnp.concatenate(weights, axis=1), two(j, 256), preferred_element_type=F32
            )
            total = part if total is None else total + part
        total = total.astype(BF16)
        o_ref[2 * i] = total[:128]
        o_ref[2 * i + 1] = total[128:]


def attend(x):
    blocks = x.shape[0]
    return pl.pallas_call(
        attend_kernel,
        out_shape=jax.ShapeDtypeStruct((blocks, 128, 128), BF16),
        in_specs=[VMEM],
        out_specs=VMEM,
        compiler_params=pltpu.CompilerParams(vmem_limit_bytes=14 << 20),
        cost_estimate=pl.CostEstimate(
            flops=12 * 10**9, bytes_accessed=3 * 10**6, transcendentals=7 * 10**6
        ),
        name="attend",
    )(x)


def route_kernel(picks_ref, rank_ref, slot_ref):
    tokens = picks_ref.shape[1]
    experts = 128
    expert = lax.broadcasted_iota(jnp.int32, (experts, tokens), 0)
    one, zero = jnp.ones((), F32), jnp.zeros((), F32)
    earlier = jnp.where(
        lax.broadcasted_iota(jnp.int32, (tokens, tokens), 0)
        < lax.broadcasted_iota(jnp.int32, (tokens, tokens), 1),
        one, zero,
    ).astype(BF16)
    number = lax.broadcasted_iota(jnp.int32, (1, tokens), 1).astype(F32)
    taken, slots = None, None
    for k in range(picks_ref.shape[0]):
        onehot = jnp.where(expert == picks_ref[k : k + 1, :], one, zero)
        before = jnp.dot(onehot.astype(BF16), earlier, preferred_element_type=F32)
        if taken is not None:
            before = before + taken
        rank = jnp.sum(onehot * before, axis=0, keepdims=True)
        count = jnp.sum(onehot, axis=1, keepdims=True)
        taken = count if taken is None else taken + count
        rank_ref[k : k + 1, :] = rank.astype(jnp.int32)
        slot = lax.broadcasted_iota(jnp.int32, (8, tokens), 0).astype(F32)
        held = jnp.where(slot == rank, number, zero).astype(BF16)
        part = lax.dot_general(
            held, onehot.astype(BF16), (((1,), (1,)), ((), ())), preferred_element_type=F32
        )
        slots = part if slots is None else slots + part
    slot_ref[...] = slots.astype(jnp.int32)


def route(picks):
    return pl.pallas_call(
        route_kernel,
        out_shape=(
            jax.ShapeDtypeStruct(picks.shape, jnp.int32),
            jax.ShapeDtypeStruct((8, 128), jnp.int32),
        ),
        in_specs=[VMEM],
        out_specs=(VMEM, VMEM),
        compiler_params=pltpu.CompilerParams(vmem_limit_bytes=4 << 20),
        cost_estimate=pl.CostEstimate(flops=2 * 10**7, bytes_accessed=10**4, transcendentals=0),
        name="route",
    )(picks)


def project_kernel(own_x_ref, other_x_ref, *refs, first_rows):
    *weights, own_ref, other_ref, w_ref, sem = refs
    copies = [
        pltpu.make_async_copy(ref, w_ref.at[k, pl.ds(0, ref.shape[0]), :], sem.at[k])
        for k, ref in enumerate(weights)
    ]
    for copy in copies:
        copy.start()
    heads = own_x_ref.shape[0]
    rows = [
        jnp.concatenate([ref[h] for h in range(heads)], axis=1) for ref in (own_x_ref, other_x_ref)
    ]
    both = jnp.concatenate(rows, axis=0)
    for k, copy in enumerate(copies):
        copy.wait()
        depth = weights[k].shape[0]
        start = 0 if first_rows is None else first_rows
        for n in range(0, 512, 256):
            out = jnp.dot(
                both[:, start : start + depth], w_ref[k, :depth, n : n + 256],
                preferred_element_type=F32,
            )
            own_ref[k, :, n : n + 256] = out[:128]
            other_ref[k, :, n : n + 256] = out[128:]


def project(own_x, other_x, weights, first_rows=None):
    count = len(weights)
    shape = jax.ShapeDtypeStruct((count, 128, 512), F32)
    return pl.pallas_call(
        functools.partial(project_kernel, first_rows=first_rows),
        out_shape=(shape, shape),
        in_specs=[VMEM, VMEM] + [ANY] * count,
        out_specs=(VMEM, VMEM),
        scratch_shapes=[
            pltpu.VMEM((count, max(w.shape[0] for w in weights), 512), BF16),
            pltpu.SemaphoreType.DMA((count,)),
        ],
        compiler_params=pltpu.CompilerParams(vmem_limit_bytes=(5 + 3 * count) << 20),
        cost_estimate=pl.CostEstimate(
            flops=count * 10**9, bytes_accessed=count * 3 * 10**6, transcendentals=0
        ),
    )(own_x, other_x, *weights)


def to_rows(inner, outer):
    i = lax.broadcasted_iota(jnp.int32, (256, 256), 0)
    k = lax.broadcasted_iota(jnp.int32, (256, 256), 1)
    return jnp.where(k == (i % inner) * outer + i // inner, 1.0, 0.0).astype(BF16)


def stack_blocks(lower, upper):
    left = jnp.concatenate([lower[:, c * 128 : c * 128 + 128] for c in range(32)], axis=0)
    right = jnp.concatenate([upper[:, c * 128 : c * 128 + 128] for c in range(32)], axis=0)
    return jnp.concatenate([left, right], axis=1)


def mix_kernel(
    slot_ref, own_ref, own_far_ref, got_ref, got_far_ref, residual_ref, mixer_ref, expert_ref,
    stream_ref, out_ref, proj_ref, rows_ref,
):
    chip, core = lax.axis_index("yh") * 2 + lax.axis_index("yl"), lax.axis_index("c")
    for member, near, far in ((core, own_ref, own_far_ref), (1 - core, got_ref, got_far_ref)):
        for k, step in enumerate((0, 3 - 2 * member, 2, 1 + 2 * member)):
            at = lax.rem(chip + step, 4) * 1024 + member * 512
            block = near[k] if k < 3 else near[k] + far[0]
            proj_ref[:, pl.ds(pl.multiple_of(at, 512), 512)] = block
    spread = to_rows(32, 8)
    width = proj_ref.shape[1]

    @pl.loop(0, proj_ref.shape[0] // 16, unroll=8)
    def _(g):
        at = pl.ds(pl.multiple_of(g * 16, 16), 16)
        p = proj_ref[at, :]
        r = lax.rsqrt(jnp.sum(p * p, axis=1, keepdims=True) * (1.0 / width) + EPSILON)
        stream = (residual_ref[at, :].astype(F32) + p * r * mixer_ref[...]).astype(BF16)
        s = stream.astype(F32)
        r = lax.rsqrt(jnp.sum(s * s, axis=1, keepdims=True) * (1.0 / width) + EPSILON)
        x = s * r * expert_ref[...]
        for value, ref in ((s, stream_ref), (x, rows_ref)):
            spread_out = jnp.dot(
                spread, stack_blocks(value[:8], value[8:]).astype(BF16), preferred_element_type=F32
            ).astype(BF16)
            ref[pl.ds(g * 16, 8)] = spread_out[:, :128].reshape(8, 32, 128)
            ref[pl.ds(g * 16 + 8, 8)] = spread_out[:, 128:].reshape(8, 32, 128)

    experts = out_ref.shape[0]

    @pl.loop(0, experts, unroll=16)
    def _(e):
        for slot in range(out_ref.shape[1] // 32):
            out_ref[e, slot * 32 : slot * 32 + 32, :] = rows_ref[slot_ref[slot, e]]


def mix(slots, projected, residual, mixer_gain, expert_gain):
    tokens, width = residual.shape
    return pl.pallas_call(
        mix_kernel,
        out_shape=(
            jax.ShapeDtypeStruct((tokens, 32, 128), BF16),
            jax.ShapeDtypeStruct((128, 96, 128), BF16),
        ),
        in_specs=[SMEM] + [VMEM] * 7,
        out_specs=(VMEM, VMEM),
        scratch_shapes=[pltpu.VMEM((tokens, width), F32), pltpu.VMEM((tokens, 32, 128), BF16)],
        compiler_params=pltpu.CompilerParams(vmem_limit_bytes=14 << 20),
        cost_estimate=pl.CostEstimate(flops=10**9, bytes_accessed=8 * 10**6, transcendentals=0),
        name="mix",
    )(slots, *projected, residual, mixer_gain, expert_gain)


def expert_kernel(x_ref, gate_ref, up_ref, down_ref, o_ref, rows_ref, hidden_ref, result_ref):
    sources = x_ref.shape[0]
    slots = x_ref.shape[1] // 32
    gather = to_rows(8, 32)
    spread = to_rows(32, 8)

    for slot in range(slots):

        @pl.loop(0, sources // 16, unroll=8)
        def _(g):
            at = slice(slot * 32, slot * 32 + 32)
            left = x_ref[pl.ds(g * 16, 8), at, :].reshape(256, 128)
            right = x_ref[pl.ds(g * 16 + 8, 8), at, :].reshape(256, 128)
            got = jnp.dot(
                gather, jnp.concatenate([left, right], axis=1), preferred_element_type=F32
            )
            to = pl.ds(pl.multiple_of(slot * sources + g * 16, 16), 16)
            for c in range(32):
                rows_ref[to, c * 128 : c * 128 + 128] = jnp.concatenate(
                    [got[c * 8 : c * 8 + 8, :128], got[c * 8 : c * 8 + 8, 128:]], axis=0
                ).astype(BF16)

    for n in range(0, 512, 256):
        a = jnp.dot(rows_ref[...], gate_ref[:, n : n + 256], preferred_element_type=F32)
        b = jnp.dot(rows_ref[...], up_ref[:, n : n + 256], preferred_element_type=F32)
        hidden_ref[:, n : n + 256] = (a / (1.0 + jnp.exp(-a)) * b).astype(BF16)

    for n in range(0, 4096, 1024):
        result_ref[:, n : n + 1024] = jnp.dot(
            hidden_ref[...], down_ref[:, n : n + 1024], preferred_element_type=F32
        )

    for slot in range(slots):

        @pl.loop(0, sources // 16, unroll=8)
        def _(g):
            base = slot * sources + g * 16
            lower = result_ref[pl.ds(pl.multiple_of(base, 8), 8), :]
            upper = result_ref[pl.ds(pl.multiple_of(base + 8, 8), 8), :]
            out = jnp.dot(
                spread, stack_blocks(lower, upper).astype(BF16), preferred_element_type=F32
            ).astype(BF16)
            at = slice(slot * 32, slot * 32 + 32)
            o_ref[pl.ds(g * 16, 8), at, :] = out[:, :128].reshape(8, 32, 128)
            o_ref[pl.ds(g * 16 + 8, 8), at, :] = out[:, 128:].reshape(8, 32, 128)


def run_experts(x, gate, up, down):
    rows = x.shape[0] * (x.shape[1] // 32)
    return pl.pallas_call(
        expert_kernel,
        out_shape=jax.ShapeDtypeStruct(x.shape, BF16),
        in_specs=[VMEM] * 4,
        out_specs=VMEM,
        scratch_shapes=[
            pltpu.VMEM((rows, 4096), BF16),
            pltpu.VMEM((rows, 512), BF16),
            pltpu.VMEM((rows, 4096), F32),
        ],
        compiler_params=pltpu.CompilerParams(vmem_limit_bytes=18 << 20),
        cost_estimate=pl.CostEstimate(flops=6 * 10**9, bytes_accessed=19 * 10**6, transcendentals=0),
        name="experts",
    )(x, gate, up, down)


def combine_kernel(
    expert_ref, rank_ref, weight_ref, x_ref, stream_ref, gain_ref, o_hbm, o_ref, sem
):
    tokens = stream_ref.shape[0]
    gather = to_rows(8, 32)
    gain = gain_ref[...]

    def one(t):
        total = None
        for k in range(2):
            rank = pl.multiple_of(rank_ref[k, t] * 32, 32)
            part = x_ref[expert_ref[k, t], pl.ds(rank, 32), :].astype(F32) * weight_ref[k, t]
            total = part if total is None else total + part
        square = jnp.sum(jnp.sum(total * total, axis=0, keepdims=True), axis=1, keepdims=True)
        r = lax.rsqrt(square * (1.0 / 4096) + EPSILON)
        return (stream_ref[t].astype(F32) + total * r * gain).astype(BF16)

    copies = []
    for chunk in range(CHUNKS):
        size = tokens // CHUNKS

        @pl.loop(0, size // 16, unroll=size // 16)
        def _(g):
            start = chunk * size + g * 16
            left = jnp.concatenate([one(start + t) for t in range(8)], axis=0)
            right = jnp.concatenate([one(start + 8 + t) for t in range(8)], axis=0)
            got = jnp.dot(gather, jnp.concatenate([left, right], axis=1), preferred_element_type=F32)
            to = pl.ds(pl.multiple_of(start, 16), 16)
            for c in range(32):
                o_ref[to, c * 128 : c * 128 + 128] = jnp.concatenate(
                    [got[c * 8 : c * 8 + 8, :128], got[c * 8 : c * 8 + 8, 128:]], axis=0
                ).astype(BF16)

        at = pl.ds(chunk * size, size)
        copy = pltpu.make_async_copy(o_ref.at[at, :], o_hbm.at[at, :], sem.at[chunk])
        copy.start()
        copies.append(copy)
    for copy in copies:
        copy.wait()


def combine(expert, rank, weight, x, stream, gain):
    tokens = stream.shape[0]
    return pl.pallas_call(
        combine_kernel,
        out_shape=jax.ShapeDtypeStruct((tokens, 4096), BF16),
        in_specs=[SMEM, SMEM, SMEM, VMEM, VMEM, VMEM],
        out_specs=pl.BlockSpec(memory_space=pl.ANY),
        scratch_shapes=[pltpu.VMEM((tokens, 4096), BF16), pltpu.SemaphoreType.DMA((CHUNKS,))],
        compiler_params=pltpu.CompilerParams(vmem_limit_bytes=14 << 20),
        cost_estimate=pl.CostEstimate(flops=10**9, bytes_accessed=6 * 10**6, transcendentals=0),
        name="combine",
    )(expert, rank, weight, x, stream, gain)


def layer(
    queries, key_rows, values, residual, out_weight, mixer_gain, expert_gain,
    gate_weight, up_weight, expert_down_matrix, routes, route_weight, output_gain,
):
    onward = [(d, (d + (2, 6)[d % 2]) % 8) for d in range(8)]
    back = [(d, (d + (6, 2)[d % 2]) % 8) for d in range(8)]
    swap = [(0, 1), (1, 0)]
    w_first = lax.ppermute(out_weight, DP, onward)
    w_far = lax.ppermute(w_first, DP, onward)
    half = out_weight.shape[0] // 2
    w_second = lax.ppermute(out_weight[:half], DP, back)
    w_last = lax.ppermute(out_weight[half:], DP, back)

    picks = jnp.transpose(routes[0])
    rank, slots = route(picks)

    packed = jnp.concatenate(
        [jnp.transpose(a[0], (1, 0, 2)) for a in (queries, key_rows, values)], axis=1
    )
    by_head = lax.all_to_all(packed, "sp", split_axis=0, concat_axis=0, tiled=True)
    attended = attend(by_head)
    own_x = lax.all_to_all(attended, "sp", split_axis=0, concat_axis=0, tiled=True)
    other_x = lax.ppermute(own_x, "c", swap)
    own, other = project(own_x, other_x, (out_weight, w_first, w_far, w_second))
    got = lax.ppermute(other, "c", swap)
    own_far, other_far = project(own_x, other_x, (w_last,), half)
    got_far = lax.ppermute(other_far, "c", swap)
    stream, outgoing = mix(
        slots, (own, own_far, got, got_far), residual[0], mixer_gain.reshape(1, -1),
        expert_gain.reshape(1, -1),
    )
    arrived = lax.all_to_all(outgoing, ALL, split_axis=0, concat_axis=0, tiled=True)
    result = run_experts(arrived, gate_weight[0], up_weight[0], expert_down_matrix[0])
    returned = lax.all_to_all(result, ALL, split_axis=0, concat_axis=0, tiled=True)
    output = combine(
        picks, rank, jnp.transpose(route_weight[0]), returned, stream, output_gain.reshape(32, 128)
    )
    return output[None]


def solution(mesh):
    mesh = Mesh(mesh.devices.reshape(16, 2, 2, 2), ALL)
    in_specs = (
        P(DP, "sp", None, None),
        P(DP, "sp", None, None),
        P(DP, "sp", None, None),
        P(DP, "sp", None),
        P(None, DP),
        P(),
        P(),
        P(ALL, None, None),
        P(ALL, None, None),
        P(ALL, None, None),
        P(DP, "sp", None),
        P(DP, "sp", None),
        P(),
    )
    return jax.shard_map(
        layer, mesh=mesh, in_specs=in_specs, out_specs=P(DP, "sp", None), check_vma=False
    )
```

```python
import functools
import math

import jax
import jax.numpy as jnp
from jax import lax
from jax.experimental import pallas as pl
from jax.experimental.pallas import tpu as pltpu
from jax.sharding import Mesh, PartitionSpec as P


EPSILON = 1e-06
F32 = jnp.float32
BF16 = jnp.bfloat16
DP = ("yh", "yl", "c")
ALL = ("sp", "yh", "yl", "c")
VMEM = pl.BlockSpec(memory_space=pltpu.VMEM)
ANY = pl.BlockSpec(memory_space=pl.ANY)
HBM = pl.BlockSpec(memory_space=pltpu.HBM)
CHUNKS = 4
SMEM = pl.BlockSpec(memory_space=pltpu.SMEM)


def attend_kernel(x_ref, o_ref):
    blocks, _, hd = x_ref.shape
    tile = 256
    scale = math.log2(math.e) * hd ** -0.5
    row = lax.broadcasted_iota(jnp.int32, (256, 256), 0) % 128
    col = lax.broadcasted_iota(jnp.int32, (256, 256), 1)
    sums = jnp.where((col >= 128) | (row > col), 1.0, 0.0).astype(BF16)
    query_pos = lax.broadcasted_iota(jnp.int32, (tile, 128), 0)
    key_pos = lax.broadcasted_iota(jnp.int32, (tile, 128), 1)

    def two(block, start):
        return jnp.concatenate(
            [x_ref[2 * block, start : start + 128], x_ref[2 * block + 1, start : start + 128]], axis=0
        )

    for i in range(blocks // 2):
        q = two(i, 0)
        carry, total = None, None
        for j in range(i, -1, -1):
            z = (
                lax.dot_general(q, two(j, 128), (((1,), (1,)), ((), ())), preferred_element_type=F32)
                * scale
            )
            weights = [None, None]
            for half in (1, 0):
                zh = z[:, half * 128 : half * 128 + 128]
                keep = jnp.maximum(zh, 0.0) + jnp.log2(1.0 + jnp.exp2(-jnp.abs(zh)))
                take = zh - keep
                if i == j:
                    past = key_pos + half * 128 < query_pos
                    keep = jnp.where(past, keep, 0.0)
                high = keep.astype(BF16)
                low = (keep - high.astype(F32)).astype(BF16)
                s = jnp.dot(jnp.concatenate([high, low], axis=1), sums, preferred_element_type=F32)
                e = take - s[:, :128]
                if carry is not None:
                    e = e - carry
                w = jnp.exp2(e)
                if i == j:
                    w = jnp.where(past, w, 0.0)
                weights[half] = w.astype(BF16)
                carry = s[:, 128:] if carry is None else carry + s[:, 128:]
            part = jnp.dot(
                jnp.concatenate(weights, axis=1), two(j, 256), preferred_element_type=F32
            )
            total = part if total is None else total + part
        total = total.astype(BF16)
        o_ref[2 * i] = total[:128]
        o_ref[2 * i + 1] = total[128:]


def attend(x):
    blocks = x.shape[0]
    return pl.pallas_call(
        attend_kernel,
        out_shape=jax.ShapeDtypeStruct((blocks, 128, 128), BF16),
        in_specs=[VMEM],
        out_specs=VMEM,
        compiler_params=pltpu.CompilerParams(vmem_limit_bytes=14 << 20),
        cost_estimate=pl.CostEstimate(
            flops=12 * 10**9, bytes_accessed=3 * 10**6, transcendentals=7 * 10**6
        ),
        name="attend",
    )(x)


def route_kernel(picks_ref, rank_ref, slot_ref):
    tokens = picks_ref.shape[1]
    experts = 128
    expert = lax.broadcasted_iota(jnp.int32, (experts, tokens), 0)
    one, zero = jnp.ones((), F32), jnp.zeros((), F32)
    earlier = jnp.where(
        lax.broadcasted_iota(jnp.int32, (tokens, tokens), 0)
        < lax.broadcasted_iota(jnp.int32, (tokens, tokens), 1),
        one, zero,
    ).astype(BF16)
    number = lax.broadcasted_iota(jnp.int32, (1, tokens), 1).astype(F32)
    taken, slots = None, None
    for k in range(picks_ref.shape[0]):
        onehot = jnp.where(expert == picks_ref[k : k + 1, :], one, zero)
        before = jnp.dot(onehot.astype(BF16), earlier, preferred_element_type=F32)
        if taken is not None:
            before = before + taken
        rank = jnp.sum(onehot * before, axis=0, keepdims=True)
        count = jnp.sum(onehot, axis=1, keepdims=True)
        taken = count if taken is None else taken + count
        rank_ref[k : k + 1, :] = rank.astype(jnp.int32)
        slot = lax.broadcasted_iota(jnp.int32, (8, tokens), 0).astype(F32)
        held = jnp.where(slot == rank, number, zero).astype(BF16)
        part = lax.dot_general(
            held, onehot.astype(BF16), (((1,), (1,)), ((), ())), preferred_element_type=F32
        )
        slots = part if slots is None else slots + part
    slot_ref[...] = slots.astype(jnp.int32)


def route(picks):
    return pl.pallas_call(
        route_kernel,
        out_shape=(
            jax.ShapeDtypeStruct(picks.shape, jnp.int32),
            jax.ShapeDtypeStruct((8, 128), jnp.int32),
        ),
        in_specs=[VMEM],
        out_specs=(VMEM, VMEM),
        compiler_params=pltpu.CompilerParams(vmem_limit_bytes=4 << 20),
        cost_estimate=pl.CostEstimate(flops=2 * 10**7, bytes_accessed=10**4, transcendentals=0),
        name="route",
    )(picks)


def project_kernel(own_x_ref, other_x_ref, *refs, first_rows):
    *weights, own_ref, other_ref, w_ref, sem = refs
    copies = [
        pltpu.make_async_copy(ref, w_ref.at[k, pl.ds(0, ref.shape[0]), :], sem.at[k])
        for k, ref in enumerate(weights)
    ]
    for copy in copies:
        copy.start()
    heads = own_x_ref.shape[0]
    rows = [
        jnp.concatenate([ref[h] for h in range(heads)], axis=1) for ref in (own_x_ref, other_x_ref)
    ]
    both = jnp.concatenate(rows, axis=0)
    for k, copy in enumerate(copies):
        copy.wait()
        depth = weights[k].shape[0]
        start = 0 if first_rows is None else first_rows
        for n in range(0, 512, 256):
            out = jnp.dot(
                both[:, start : start + depth], w_ref[k, :depth, n : n + 256],
                preferred_element_type=F32,
            )
            own_ref[k, :, n : n + 256] = out[:128]
            other_ref[k, :, n : n + 256] = out[128:]


def project(own_x, other_x, weights, first_rows=None):
    count = len(weights)
    shape = jax.ShapeDtypeStruct((count, 128, 512), F32)
    return pl.pallas_call(
        functools.partial(project_kernel, first_rows=first_rows),
        out_shape=(shape, shape),
        in_specs=[VMEM, VMEM] + [ANY] * count,
        out_specs=(VMEM, VMEM),
        scratch_shapes=[
            pltpu.VMEM((count, max(w.shape[0] for w in weights), 512), BF16),
            pltpu.SemaphoreType.DMA((count,)),
        ],
        compiler_params=pltpu.CompilerParams(vmem_limit_bytes=(5 + 3 * count) << 20),
        cost_estimate=pl.CostEstimate(
            flops=count * 10**9, bytes_accessed=count * 3 * 10**6, transcendentals=0
        ),
    )(own_x, other_x, *weights)


def to_rows(inner, outer):
    i = lax.broadcasted_iota(jnp.int32, (256, 256), 0)
    k = lax.broadcasted_iota(jnp.int32, (256, 256), 1)
    return jnp.where(k == (i % inner) * outer + i // inner, 1.0, 0.0).astype(BF16)


def stack_blocks(lower, upper):
    left = jnp.concatenate([lower[:, c * 128 : c * 128 + 128] for c in range(32)], axis=0)
    right = jnp.concatenate([upper[:, c * 128 : c * 128 + 128] for c in range(32)], axis=0)
    return jnp.concatenate([left, right], axis=1)


def mix_kernel(
    slot_ref, own_ref, own_far_ref, got_ref, got_far_ref, residual_ref, mixer_ref, expert_ref,
    stream_ref, out_ref, proj_ref, rows_ref,
):
    chip, core = lax.axis_index("yh") * 2 + lax.axis_index("yl"), lax.axis_index("c")
    for member, near, far in ((core, own_ref, own_far_ref), (1 - core, got_ref, got_far_ref)):
        for k, step in enumerate((0, 3 - 2 * member, 1 + 2 * member, 2)):
            at = lax.rem(chip + step, 4) * 1024 + member * 512
            block = near[k] if k < 3 else near[k] + far[0]
            proj_ref[:, pl.ds(pl.multiple_of(at, 512), 512)] = block
    spread = to_rows(32, 8)
    width = proj_ref.shape[1]

    @pl.loop(0, proj_ref.shape[0] // 16, unroll=8)
    def _(g):
        at = pl.ds(pl.multiple_of(g * 16, 16), 16)
        p = proj_ref[at, :]
        r = lax.rsqrt(jnp.sum(p * p, axis=1, keepdims=True) * (1.0 / width) + EPSILON)
        stream = (residual_ref[at, :].astype(F32) + p * r * mixer_ref[...]).astype(BF16)
        s = stream.astype(F32)
        r = lax.rsqrt(jnp.sum(s * s, axis=1, keepdims=True) * (1.0 / width) + EPSILON)
        x = s * r * expert_ref[...]
        for value, ref in ((s, stream_ref), (x, rows_ref)):
            spread_out = jnp.dot(
                spread, stack_blocks(value[:8], value[8:]).astype(BF16), preferred_element_type=F32
            ).astype(BF16)
            ref[pl.ds(g * 16, 8)] = spread_out[:, :128].reshape(8, 32, 128)
            ref[pl.ds(g * 16 + 8, 8)] = spread_out[:, 128:].reshape(8, 32, 128)

    experts = out_ref.shape[0]

    @pl.loop(0, experts, unroll=16)
    def _(e):
        for slot in range(out_ref.shape[1] // 32):
            out_ref[e, slot * 32 : slot * 32 + 32, :] = rows_ref[slot_ref[slot, e]]


def mix(slots, projected, residual, mixer_gain, expert_gain):
    tokens, width = residual.shape
    return pl.pallas_call(
        mix_kernel,
        out_shape=(
            jax.ShapeDtypeStruct((tokens, 32, 128), BF16),
            jax.ShapeDtypeStruct((128, 96, 128), BF16),
        ),
        in_specs=[SMEM] + [VMEM] * 7,
        out_specs=(VMEM, VMEM),
        scratch_shapes=[pltpu.VMEM((tokens, width), F32), pltpu.VMEM((tokens, 32, 128), BF16)],
        compiler_params=pltpu.CompilerParams(vmem_limit_bytes=14 << 20),
        cost_estimate=pl.CostEstimate(flops=10**9, bytes_accessed=8 * 10**6, transcendentals=0),
        name="mix",
    )(slots, *projected, residual, mixer_gain, expert_gain)


def expert_kernel(x_ref, gate_ref, up_ref, down_ref, o_ref, rows_ref, hidden_ref, result_ref):
    sources = x_ref.shape[0]
    slots = x_ref.shape[1] // 32
    gather = to_rows(8, 32)
    spread = to_rows(32, 8)

    for slot in range(slots):

        @pl.loop(0, sources // 16, unroll=8)
        def _(g):
            at = slice(slot * 32, slot * 32 + 32)
            left = x_ref[pl.ds(g * 16, 8), at, :].reshape(256, 128)
            right = x_ref[pl.ds(g * 16 + 8, 8), at, :].reshape(256, 128)
            got = jnp.dot(
                gather, jnp.concatenate([left, right], axis=1), preferred_element_type=F32
            )
            to = pl.ds(pl.multiple_of(slot * sources + g * 16, 16), 16)
            for c in range(32):
                rows_ref[to, c * 128 : c * 128 + 128] = jnp.concatenate(
                    [got[c * 8 : c * 8 + 8, :128], got[c * 8 : c * 8 + 8, 128:]], axis=0
                ).astype(BF16)

    for n in range(0, 512, 256):
        a = jnp.dot(rows_ref[...], gate_ref[:, n : n + 256], preferred_element_type=F32)
        b = jnp.dot(rows_ref[...], up_ref[:, n : n + 256], preferred_element_type=F32)
        hidden_ref[:, n : n + 256] = (a / (1.0 + jnp.exp(-a)) * b).astype(BF16)

    for n in range(0, 4096, 1024):
        result_ref[:, n : n + 1024] = jnp.dot(
            hidden_ref[...], down_ref[:, n : n + 1024], preferred_element_type=F32
        )

    for slot in range(slots):

        @pl.loop(0, sources // 16, unroll=8)
        def _(g):
            base = slot * sources + g * 16
            lower = result_ref[pl.ds(pl.multiple_of(base, 8), 8), :]
            upper = result_ref[pl.ds(pl.multiple_of(base + 8, 8), 8), :]
            out = jnp.dot(
                spread, stack_blocks(lower, upper).astype(BF16), preferred_element_type=F32
            ).astype(BF16)
            at = slice(slot * 32, slot * 32 + 32)
            o_ref[pl.ds(g * 16, 8), at, :] = out[:, :128].reshape(8, 32, 128)
            o_ref[pl.ds(g * 16 + 8, 8), at, :] = out[:, 128:].reshape(8, 32, 128)


def run_experts(x, gate, up, down):
    rows = x.shape[0] * (x.shape[1] // 32)
    return pl.pallas_call(
        expert_kernel,
        out_shape=jax.ShapeDtypeStruct(x.shape, BF16),
        in_specs=[VMEM] * 4,
        out_specs=VMEM,
        scratch_shapes=[
            pltpu.VMEM((rows, 4096), BF16),
            pltpu.VMEM((rows, 512), BF16),
            pltpu.VMEM((rows, 4096), F32),
        ],
        compiler_params=pltpu.CompilerParams(vmem_limit_bytes=18 << 20),
        cost_estimate=pl.CostEstimate(flops=6 * 10**9, bytes_accessed=19 * 10**6, transcendentals=0),
        name="experts",
    )(x, gate, up, down)


def combine_kernel(
    expert_ref, rank_ref, weight_ref, x_ref, stream_ref, gain_ref, o_hbm, o_ref, sem
):
    tokens = stream_ref.shape[0]
    gather = to_rows(8, 32)
    gain = gain_ref[...]

    def one(t):
        total = None
        for k in range(2):
            rank = pl.multiple_of(rank_ref[k, t] * 32, 32)
            part = x_ref[expert_ref[k, t], pl.ds(rank, 32), :].astype(F32) * weight_ref[k, t]
            total = part if total is None else total + part
        square = jnp.sum(jnp.sum(total * total, axis=0, keepdims=True), axis=1, keepdims=True)
        r = lax.rsqrt(square * (1.0 / 4096) + EPSILON)
        return (stream_ref[t].astype(F32) + total * r * gain).astype(BF16)

    copies = []
    for chunk in range(CHUNKS):
        size = tokens // CHUNKS

        @pl.loop(0, size // 16, unroll=size // 16)
        def _(g):
            start = chunk * size + g * 16
            left = jnp.concatenate([one(start + t) for t in range(8)], axis=0)
            right = jnp.concatenate([one(start + 8 + t) for t in range(8)], axis=0)
            got = jnp.dot(gather, jnp.concatenate([left, right], axis=1), preferred_element_type=F32)
            to = pl.ds(pl.multiple_of(start, 16), 16)
            for c in range(32):
                o_ref[to, c * 128 : c * 128 + 128] = jnp.concatenate(
                    [got[c * 8 : c * 8 + 8, :128], got[c * 8 : c * 8 + 8, 128:]], axis=0
                ).astype(BF16)

        at = pl.ds(chunk * size, size)
        copy = pltpu.make_async_copy(o_ref.at[at, :], o_hbm.at[at, :], sem.at[chunk])
        copy.start()
        copies.append(copy)
    for copy in copies:
        copy.wait()


def combine(expert, rank, weight, x, stream, gain):
    tokens = stream.shape[0]
    return pl.pallas_call(
        combine_kernel,
        out_shape=jax.ShapeDtypeStruct((tokens, 4096), BF16),
        in_specs=[SMEM, SMEM, SMEM, VMEM, VMEM, VMEM],
        out_specs=pl.BlockSpec(memory_space=pl.ANY),
        scratch_shapes=[pltpu.VMEM((tokens, 4096), BF16), pltpu.SemaphoreType.DMA((CHUNKS,))],
        compiler_params=pltpu.CompilerParams(vmem_limit_bytes=14 << 20),
        cost_estimate=pl.CostEstimate(flops=10**9, bytes_accessed=6 * 10**6, transcendentals=0),
        name="combine",
    )(expert, rank, weight, x, stream, gain)


def layer(
    queries, key_rows, values, residual, out_weight, mixer_gain, expert_gain,
    gate_weight, up_weight, expert_down_matrix, routes, route_weight, output_gain,
):
    onward = [(d, (d + (2, 6)[d % 2]) % 8) for d in range(8)]
    back = [(d, (d + (6, 2)[d % 2]) % 8) for d in range(8)]
    swap = [(0, 1), (1, 0)]
    w_first = lax.ppermute(out_weight, DP, onward)
    w_second = lax.ppermute(out_weight, DP, back)
    half = out_weight.shape[0] // 2
    w_far = lax.ppermute(w_first[:half], DP, onward)
    w_last = lax.ppermute(w_first[half:], DP, onward)

    picks = jnp.transpose(routes[0])
    rank, slots = route(picks)

    packed = jnp.concatenate(
        [jnp.transpose(a[0], (1, 0, 2)) for a in (queries, key_rows, values)], axis=1
    )
    by_head = lax.all_to_all(packed, "sp", split_axis=0, concat_axis=0, tiled=True)
    attended = attend(by_head)
    own_x = lax.all_to_all(attended, "sp", split_axis=0, concat_axis=0, tiled=True)
    other_x = lax.ppermute(own_x, "c", swap)
    own, other = project(own_x, other_x, (out_weight, w_first, w_second, w_far))
    got = lax.ppermute(other, "c", swap)
    own_far, other_far = project(own_x, other_x, (w_last,), half)
    got_far = lax.ppermute(other_far, "c", swap)
    stream, outgoing = mix(
        slots, (own, own_far, got, got_far), residual[0], mixer_gain.reshape(1, -1),
        expert_gain.reshape(1, -1),
    )
    arrived = lax.all_to_all(outgoing, ALL, split_axis=0, concat_axis=0, tiled=True)
    result = run_experts(arrived, gate_weight[0], up_weight[0], expert_down_matrix[0])
    returned = lax.all_to_all(result, ALL, split_axis=0, concat_axis=0, tiled=True)
    output = combine(
        picks, rank, jnp.transpose(route_weight[0]), returned, stream, output_gain.reshape(32, 128)
    )
    return output[None]


def solution(mesh):
    mesh = Mesh(mesh.devices.reshape(16, 2, 2, 2), ALL)
    in_specs = (
        P(DP, "sp", None, None),
        P(DP, "sp", None, None),
        P(DP, "sp", None, None),
        P(DP, "sp", None),
        P(None, DP),
        P(),
        P(),
        P(ALL, None, None),
        P(ALL, None, None),
        P(ALL, None, None),
        P(DP, "sp", None),
        P(DP, "sp", None),
        P(),
    )
    return jax.shard_map(
        layer, mesh=mesh, in_specs=in_specs, out_specs=P(DP, "sp", None), check_vma=False
    )
```
